32 devices in a mesh: grp: 2 (over y), sp: 4 (over z), tp: 4 (over x, core).
Axes of the slice: x: 2, y: 2, z: 4, core: 2. Of those that a mesh axis runs over, the one named last changes fastest.
Arguments:
- conv_value: bfloat16 [4096, 1024], P(('grp', 'sp'), 'tp'), parts along dimension 0, may hold values from -6 to 6
- conv_gate: bfloat16 [4096, 1024], P(('grp', 'sp'), 'tp'), parts along dimension 0, may hold values from -6 to 6
- kernel: bfloat16 [31, 1024], P(None, 'tp'), may hold values from -4 to 4
- conv_bias: float32 [1024], P('tp'), may hold values from -3 to 3
- ln_gain: float32 [1024], P('tp'), may hold values from 0.1 to 1.9
- ln_bias: float32 [1024], P('tp'), may hold values from -3 to 3
- out_gain: float32 [1024], P('tp'), may hold values from 0.1 to 1.9
- out_weight: bfloat16 [1024, 2048], replicated, may hold values from -0.1875 to 0.1875
- residual: bfloat16 [4096, 2048], P(('grp', 'sp', 'tp')), parts along dimension 0, may hold values from -6 to 6
- moe_gain: float32 [2048], replicated, may hold values from 0.1 to 1.9
- expert_ids: int32 [4096, 2], P(('grp', 'sp', 'tp')), parts along dimension 0, may hold values from 0 to 15, as said below
- expert_weights: float32 [4096, 2], P(('grp', 'sp', 'tp')), parts along dimension 0, may hold values from 0.1 to 0.7
- w_gate: bfloat16 [16, 2048, 512], P(('sp', 'tp')), may hold values from -0.125 to 0.125
- w_up: bfloat16 [16, 2048, 512], P(('sp', 'tp')), may hold values from -0.125 to 0.125
- w_down: bfloat16 [16, 512, 2048], P(('sp', 'tp')), may hold values from -0.25 to 0.25
Outputs:
- layer_out: bfloat16 [4096, 2048], P(('grp', 'sp', 'tp')), parts along dimension 0
The draws below stay inside these ranges and needn't reach their ends.
There are 2 independent parts, one for each index of `grp`. The reference program is written for one: setup_inputs(seed, part) draws one part's arguments, and reference() takes and returns one part's arrays. A program takes and returns all parts, laid end to end along the dimension named above; an argument that names none is the same for every part. Nothing has to cross between parts.
Inputs may be any that keep to these rules, and one draw needn't show every extreme that they name: `expert_ids`: each row names two different experts of one group (group = expert number // 4). Among the 128 rows of one device (aligned blocks of 128 rows) no expert is named more than 32 times, and in every such block some expert is named exactly 32 times.
All inputs are finite; a program needn't handle non-finite values.
Results may differ from the reference program's by a relative error of at most 0.0095.
Values may be sent and summed in bfloat16 or wider, within the bound.
A program may use at most 64 MiB of HBM per device.

```python
import jax
import jax.numpy as jnp
from jax import lax

D = 2048
CONV_CH = 1024
KERNEL = 31
HID = 512
ROWS = 128
TOKENS = 2048
EXPERTS = 16
EPG = 4
CAP = 32


def draw_kernel(key, part):
    key_base, key_jitter = jax.random.split(jax.random.fold_in(key, 11))
    ramp = jnp.exp(jnp.log(0.3) + jnp.log(10.0) * jnp.arange(CONV_CH, dtype=jnp.float32) / CONV_CH)
    jitter = jnp.exp(jax.random.uniform(key_jitter, (CONV_CH,), jnp.float32, -0.35, 0.35))
    base = jnp.clip(jax.random.normal(key_base, (KERNEL, CONV_CH), jnp.float32), -4.0, 4.0)
    return (base * ramp * jitter / jnp.sqrt(jnp.float32(KERNEL))).astype(jnp.bfloat16)


def draw_expert_ids(key, part):
    group_size = min(ROWS, EXPERTS // 2)
    rounds = TOKENS // group_size
    busiest = jax.random.randint(jax.random.fold_in(key, 21), (), 0, EXPERTS)
    round_keys = jax.random.split(jax.random.fold_in(key, 22), rounds)
    numbers = jnp.arange(EXPERTS, dtype=jnp.int32)

    def one_round(round_key):
        key_shift, key_order, key_mix, key_swap = jax.random.split(round_key, 4)
        shift_by = jax.random.randint(key_shift, (), 1, EPG)
        pre_image = busiest // EPG * EPG + (busiest % EPG - shift_by) % EPG
        scores = jax.random.permutation(key_order, EXPERTS).astype(jnp.int32)
        forced = (numbers == busiest) | (numbers == pre_image)
        scores = jnp.where(forced, scores + EXPERTS, scores)
        _, chosen = lax.top_k(scores, group_size)
        chosen = jax.random.permutation(key_mix, chosen.astype(jnp.int32))
        second = chosen // EPG * EPG + (chosen % EPG + shift_by) % EPG
        swapped = jax.random.randint(key_swap, (group_size,), 0, 2)
        first_col = jnp.where(swapped == 1, second, chosen)
        second_col = jnp.where(swapped == 1, chosen, second)
        return jnp.stack([first_col, second_col], axis=1).astype(jnp.int32)
    return jax.vmap(one_round)(round_keys).reshape(TOKENS, 2).astype(jnp.int32)


def block_levels(own_key, extent, shards, low, largest):
    def one(dim, shards_of):
        steps = jax.random.uniform(jax.random.fold_in(jax.random.fold_in(own_key, 6), dim), (shards_of,), jnp.float32, low / len(shards), largest / len(shards))
        return jnp.repeat(jnp.exp(steps), extent[dim] // shards_of).reshape((-1,) + (1,) * (len(extent) - dim - 1))

    level = one(*shards[0])
    for cut in shards[1:]:
        level = level * one(*cut)
    return level


def noise(stream_key, extent, scale, bound, shards=(), kind=jnp.bfloat16):
    array = scale * jax.random.normal(stream_key, extent, jnp.float32)
    if shards:
        array = array * block_levels(stream_key, extent, shards, -0.22, 0.18)
    return jnp.clip(array, -bound, bound).astype(kind)


def setup_inputs(seed: int = 0, part: int = 0) -> dict:
    keys = jax.random.split(jax.random.key(seed), 16)
    own_keys = jax.random.split(jax.random.fold_in(keys[15], part), 16)
    conv_value = noise(own_keys[0], (TOKENS, CONV_CH), 1.0, 6.0, ((0, 4), (1, 4)))
    conv_gate = noise(own_keys[1], (TOKENS, CONV_CH), 1.0, 6.0, ((0, 4), (1, 4)))
    kernel = draw_kernel(jax.random.fold_in(keys[15], 71), part)
    conv_bias = noise(keys[3], (CONV_CH,), 0.5, 3.0, ((0, 4),), jnp.float32)
    ln_gain = jnp.clip(1.0 + 0.18 * jax.random.normal(keys[4], (CONV_CH,), jnp.float32), 0.1, 1.9)
    ln_bias = noise(keys[5], (CONV_CH,), 0.5, 3.0, ((0, 4),), jnp.float32)
    out_gain = jnp.clip(1.0 + 0.18 * jax.random.normal(keys[6], (CONV_CH,), jnp.float32), 0.1, 1.9)
    out_weight = noise(keys[7], (CONV_CH, D), CONV_CH ** -0.5, 0.1875)
    residual = noise(own_keys[8], (TOKENS, D), 1.0, 6.0, ((0, 16),))
    moe_gain = jnp.clip(1.0 + 0.18 * jax.random.normal(keys[9], (D,), jnp.float32), 0.1, 1.9)
    expert_ids = draw_expert_ids(jax.random.fold_in(jax.random.fold_in(keys[15], part), 71), part)
    expert_weights = jnp.clip(0.1 + 0.59999999 * jax.random.uniform(own_keys[11], (TOKENS, 2), jnp.float32) ** block_levels(own_keys[11], (TOKENS, 2), ((0, 16),), -0.2, 0.2), 0.1, 0.7)
    w_gate = noise(keys[12], (EXPERTS, D, HID), D ** -0.5, 0.125, ((0, 16),))
    w_up = noise(keys[13], (EXPERTS, D, HID), D ** -0.5, 0.125, ((0, 16),))
    w_down = noise(keys[14], (EXPERTS, HID, D), HID ** -0.5, 0.25, ((0, 16),))
    return dict(conv_value=conv_value, conv_gate=conv_gate, kernel=kernel, conv_bias=conv_bias, ln_gain=ln_gain, ln_bias=ln_bias, out_gain=out_gain, out_weight=out_weight, residual=residual, moe_gain=moe_gain, expert_ids=expert_ids, expert_weights=expert_weights, w_gate=w_gate, w_up=w_up, w_down=w_down)


EPSILON = 1e-06

def reference(conv_value, conv_gate, kernel, conv_bias, ln_gain, ln_bias, out_gain, out_weight, residual, moe_gain, expert_ids, expert_weights, w_gate, w_up, w_down):
    gated = (conv_value.astype(jnp.float32) * jax.nn.sigmoid(conv_gate.astype(jnp.float32))).astype(jnp.bfloat16)
    padded = jnp.concatenate([jnp.zeros((KERNEL - 1, CONV_CH), gated.dtype), gated], axis=0)
    convolved = jnp.zeros((TOKENS, CONV_CH), jnp.float32) + conv_bias
    for offset in range(KERNEL):
        convolved = convolved + padded[offset:offset + TOKENS].astype(jnp.float32) * kernel[offset].astype(jnp.float32)
    average = lax.optimization_barrier(jnp.mean(convolved, axis=1, keepdims=True))
    spread = lax.optimization_barrier(jnp.mean(convolved * convolved, axis=1, keepdims=True)) - average * average
    swished = jax.nn.silu((convolved - average) * lax.rsqrt(spread + EPSILON) * ln_gain + ln_bias)
    energy = lax.optimization_barrier(jnp.mean(swished * swished, axis=1, keepdims=True))
    branch = (swished * lax.rsqrt(energy + EPSILON) * out_gain).astype(jnp.bfloat16)
    projected = jnp.dot(branch, out_weight, preferred_element_type=jnp.float32)
    hidden = (residual.astype(jnp.float32) + projected).astype(jnp.bfloat16)
    widened = hidden.astype(jnp.float32)
    normed = (widened * lax.rsqrt(lax.optimization_barrier(jnp.mean(widened * widened, axis=1, keepdims=True)) + EPSILON) * moe_gain).astype(jnp.bfloat16)
    flat_ids = expert_ids.reshape(-1).astype(jnp.int32)
    onehot = (flat_ids[:, None] == jnp.arange(EXPERTS, dtype=jnp.int32)[None, :]).astype(jnp.int32)
    slot_rank = lax.optimization_barrier(jnp.sum((jnp.cumsum(onehot, axis=0) - 1) * onehot, axis=1)).astype(jnp.int32)
    capacity = TOKENS // ROWS * CAP
    position = flat_ids * capacity + slot_rank
    token_index = (jnp.arange(2 * TOKENS, dtype=jnp.int32) // 2).astype(jnp.int32)
    table = jnp.full((EXPERTS * capacity,), TOKENS, jnp.int32).at[position].set(token_index).reshape(EXPERTS, capacity)
    weight_table = jnp.zeros((EXPERTS * capacity,), jnp.float32).at[position].set(expert_weights.reshape(-1).astype(jnp.float32)).reshape(EXPERTS, capacity)
    source_rows = jnp.concatenate([normed, jnp.zeros((1, D), normed.dtype)], axis=0)

    def one_expert(total, pieces):
        rows_index, row_weights, gate_w, up_w, down_w = pieces
        taken = source_rows[rows_index]
        gate_part = jnp.dot(taken, gate_w, preferred_element_type=jnp.float32)
        up_part = jnp.dot(taken, up_w, preferred_element_type=jnp.float32)
        active = (jax.nn.silu(gate_part) * up_part).astype(jnp.bfloat16)
        result = jnp.dot(active, down_w, preferred_element_type=jnp.float32).astype(jnp.bfloat16)
        return (total.at[rows_index].add(row_weights[:, None] * result.astype(jnp.float32)), None)
    start_total = jnp.zeros((TOKENS + 1, D), jnp.float32)
    combined, _ = lax.scan(one_expert, start_total, (table, weight_table, w_gate, w_up, w_down))
    return (widened + combined[:TOKENS]).astype(jnp.bfloat16)
```

```python
import jax
import jax.numpy as jnp
from jax import lax
from jax.experimental import pallas as pl
from jax.experimental.pallas import tpu as pltpu
from jax.sharding import PartitionSpec as P

EPSILON = 1e-06
GROUPS = 4
SPLIT = 2
LANES = 128
SUBLANES = 8
MESH = pl.DeviceIdType.MESH
COLUMNS, LATE = (2, 5, 1, 0, 3, 4, 6, 7), 4
OUTER, OUTER_PARTS = (6, 3, 4, 2, 5, 7), 1
INNER, INNER_PARTS = (3, 6, 4, 7, 2, 5), 2
PLAN = (
    "f1 z6 x0 z3",
    "m0 c0 x6 z4",
    "c6 z2 h6 b6",
    "x1 x4 c4 x3",
    "z7 c3 e6 z5",
    "h4 x2 c1 x7",
    "b4 c7 h3 h0",
    "h1 b3 x5 h7",
    "b7 e4 c2 c5",
    "h2 h5 b5 b2",
    "b1 b0 e3 e7",
    "e5 e2 e1 e0",
)


def flipped(index, mask, size):
    total, bit = 0, 1
    while bit < size:
        total = total + ((index // bit + mask // bit) % 2) * bit
        bit *= 2
    return total


def gray(index):
    return flipped(index, index // 2, 4)


def layer_kernel(
    value_hbm, gate_hbm_in, kernel_hbm, bias_hbm, lgain_hbm, lbias_hbm, ogain_hbm, res_hbm, mgain_hbm, ids_hbm, shares_hbm,
    out_hbm, gate_hbm, up_hbm, down_hbm, result,
    value, gate, kernel, params, residual, moe_gain, ids, shares,
    w_out, w_gate, w_up, w_down, taps, meta, pick, unpick, padded, halo_out, halo_in, conv, wide, gains, branch, hid,
    send, back, rows, normed, weights, own, half_out, half_in, cross_out, cross_in, final, act, total,
    load_sem, in_sem, meta_s, meta_r, halo_s, halo_r, gain_s, gain_r, group_s, group_r,
    z_s, z_r, pair_s, pair_r, x_s, x_r, via_s, via_r,
    half_s, half_r, cross_s, cross_r, back_s, back_r,
):
    spn, tpn = weights.shape[:2]
    pieces, _, height, width = rows.shape
    cap = height * SPLIT
    last = pieces - 1
    me_z, me_t = lax.axis_index("sp"), lax.axis_index("tp")
    pair, across = flipped(me_t, 1, tpn), flipped(me_t, 2, tpn)
    hidden = w_gate.shape[1]
    tok_rows, channels = value.shape
    row_count = tok_rows // tpn
    full = channels * tpn
    reach = padded.shape[0] - tok_rows
    tap_count = kernel.shape[0]
    f32, bf = jnp.float32, jnp.bfloat16

    def to(z, t):
        return {"sp": z, "tp": t}

    def copy(src, dst, s, r, z, t):
        return pltpu.make_async_remote_copy(
            src_ref=src, dst_ref=dst, send_sem=s, recv_sem=r, device_id=to(z, t), device_id_type=MESH
        )

    peers = [(q, r) for q in range(spn) for r in range(tpn) if q or r]
    barrier = pltpu.get_barrier_semaphore()
    for q, r in peers:
        pl.semaphore_signal(
            barrier, inc=1, device_id=to(flipped(me_z, gray(q), spn), flipped(me_t, r, tpn)), device_id_type=MESH
        )

    inputs = [
        pltpu.make_async_copy(a, b, in_sem.at[i])
        for i, (a, b) in enumerate((
            (value_hbm, value), (gate_hbm_in, gate), (kernel_hbm, kernel), (bias_hbm, params.at[pl.ds(3, 1)]),
            (lgain_hbm, params.at[pl.ds(0, 1)]), (lbias_hbm, params.at[pl.ds(1, 1)]),
            (ogain_hbm, params.at[pl.ds(2, 1)]), (ids_hbm, ids), (shares_hbm, shares),
            (res_hbm, residual), (mgain_hbm, moe_gain),
        ))
    ]
    loads = [
        pltpu.make_async_copy(a, b, load_sem.at[i])
        for i, (a, b) in enumerate(((out_hbm, w_out), (gate_hbm, w_gate), (up_hbm, w_up), (down_hbm, w_down)))
    ]
    for load in inputs + loads:
        load.start()

    for load in inputs[:7]:
        load.wait()
    taps[:tap_count, :] = kernel[...].astype(f32)
    gated = (value[...].astype(f32) / (1.0 + jnp.exp(-gate[...].astype(f32)))).astype(bf)
    padded[reach:, :] = gated.astype(f32)
    halo_out[...] = gated[tok_rows - reach :]

    mine = pl.ds(pl.multiple_of(me_t * channels, channels), channels)

    def halo_copy(z):
        return copy(halo_out, halo_in, halo_s.at[0], halo_r.at[0], z, me_t)

    def gain_copy(r):
        return copy(params, gains.at[:, mine], gain_s.at[r], gain_r.at[r], me_z, flipped(me_t, r, tpn))

    def group_copy(t, low, high):
        span = pl.ds(low, high - low)
        r = flipped(me_t, t, tpn)
        return copy(conv.at[t, span], wide.at[span, mine], group_s.at[r], group_r.at[r], me_z, t)

    def z_copy(k, cols=pl.ds(0, width)):
        return copy(
            send.at[k, :, cols], rows.at[k, 0, :, cols], z_s.at[k], z_r.at[k],
            flipped(me_z, gray(k // SPLIT), spn), me_t,
        )

    def meta_copy(q, r):
        return copy(
            meta.at[q], weights.at[q, r], meta_s.at[q, r], meta_r.at[q, r],
            flipped(me_z, gray(q), spn), flipped(me_t, r, tpn),
        )

    def pair_copy(k):
        return copy(rows.at[k, 0], rows.at[k, 1], pair_s.at[k], pair_r.at[k], me_z, pair)

    def x_copy(k, cols=pl.ds(0, width)):
        return copy(
            rows.at[k, 0, :, cols], rows.at[k, 2, :, cols], x_s.at[k], x_r.at[k], me_z, across
        )

    def via_copy(k):
        return copy(rows.at[k, 2], rows.at[k, 3], via_s.at[k], via_r.at[k], me_z, pair)

    def half_copy(k):
        return copy(half_out.at[k], half_in.at[k], half_s.at[k], half_r.at[k], me_z, pair)

    def cross_copy(k):
        return copy(cross_out.at[k], cross_in.at[k], cross_s.at[k], cross_r.at[k], me_z, across)

    def back_copy(k):
        return copy(
            final.at[k], back.at[COLUMNS.index(k)], back_s.at[k], back_r.at[k], flipped(me_z, gray(k // SPLIT), spn), me_t
        )

    def convolve(block, first, count):
        start = pl.multiple_of(block * row_count + first, SUBLANES)
        for c in range(0, channels, LANES):
            window = padded[pl.ds(start, count + reach), c : c + LANES]
            sums = jnp.zeros((count, LANES), f32) + params[3:4, c : c + LANES]
            for b in range(SUBLANES):
                extent = count + (SUBLANES if b else 0)
                group = None
                for a in range(0, reach + 1, SUBLANES):
                    tap = a + b - (reach - tap_count + 1)
                    if 0 <= tap < tap_count:
                        term = window[a : a + extent] * taps[tap : tap + 1, c : c + LANES]
                        group = term if group is None else group + term
                sums = sums + group[b : b + count]
            conv[block, first : first + count, c : c + LANES] = sums.astype(bf)

    side = me_t // 2
    for j, b in enumerate((2, 3, 1, 0)):
        block = b + side * (3 - 2 * b)
        edge = b in (0, 3)
        convolve(block, reach, row_count - reach)
        if edge:
            @pl.when(block != 0)
            def _():
                convolve(block, 0, reach)
        else:
            convolve(block, 0, reach)
        if j == 0:
            pl.semaphore_wait(barrier, len(peers))

            @pl.when(me_z < spn - 1)
            def _():
                halo_copy(me_z + 1).start()

            for r in range(1, tpn):
                gain_copy(r).start()

        if edge:
            @pl.when((block != me_t) & (block != 0))
            def _():
                group_copy(block, 0, row_count).start()

            @pl.when((block != me_t) & (block == 0))
            def _():
                group_copy(block, reach, row_count).start()
        else:
            @pl.when(block != me_t)
            def _():
                group_copy(block, 0, row_count).start()

    @pl.when(me_z == 0)
    def _():
        padded[:reach, :] = jnp.zeros((reach, channels), f32)

    @pl.when(me_z > 0)
    def _():
        halo_copy(me_z - 1).wait_recv()
        padded[:reach, :] = halo_in[...].astype(f32)

    convolve(0, 0, reach)

    @pl.when(me_t != 0)
    def _():
        group_copy(0, 0, reach).start()

    wide[:, mine] = conv[me_t]
    gains[:, mine] = params[...]

    for load in inputs[7:9]:
        load.wait()
    square = (row_count, row_count)
    down, along = (lax.broadcasted_iota(jnp.int32, square, d) for d in (0, 1))

    def upright(line):
        return jnp.sum(
            jnp.where(down == along, jnp.broadcast_to(line, square), jnp.zeros((), line.dtype)),
            axis=1, keepdims=True,
        )

    def distance(number):
        mask = jnp.bitwise_xor(number, me_z)
        return jnp.bitwise_xor(mask, lax.div(mask, 2))

    def place(number, order):
        found = distance(number) * SPLIT + lax.div(order, height)
        column = sum(jnp.where(found == k, c, 0) for c, k in enumerate(COLUMNS))
        return column * height + lax.rem(order, height)

    group_row = jnp.broadcast_to(lax.div(ids[0:1, :], tpn), square)
    group = jnp.broadcast_to(upright(group_row[0:1, :]), square)
    same = group == group_row
    rank = jnp.sum(jnp.where(same & (along < down), 1, 0), axis=1, keepdims=True)
    rank_row = jnp.sum(jnp.where(same & (down < along), 1, 0), axis=0, keepdims=True)
    slot = place(group[:, 0:1], rank)
    slot_row = place(group_row[0:1, :], rank_row)
    slots = spn * cap
    pick[...] = jnp.where(
        lax.broadcasted_iota(jnp.int32, (slots, row_count), 0) == slot_row, 1.0, 0.0
    ).astype(bf)
    unpick[...] = jnp.where(
        lax.broadcasted_iota(jnp.int32, (row_count, slots), 1) == slot, 1.0, 0.0
    ).astype(bf)
    lane = lax.broadcasted_iota(jnp.int32, (row_count, LANES), 1)
    experts = lax.rem(ids[...], tpn)
    meta[...] = jnp.zeros_like(meta)
    by_expert = [
        upright(jnp.sum(jnp.where(experts == e, shares[...], 0.0), axis=0, keepdims=True))
        for e in range(tpn)
    ]
    for q in range(spn):
        here = (distance(group[:, 0:1]) == q) & (lane == rank)
        for e in range(tpn):
            share = by_expert[e]
            meta[q, e : e + 1, :] = jnp.sum(jnp.where(here, share, 0.0), axis=0, keepdims=True)
    weights[0, 0] = meta[0]
    for q, r in peers:
        meta_copy(q, r).start()

    for load in inputs[9:]:
        load.wait()
    loads[0].wait()
    for r in range(1, tpn):
        gain_copy(r).wait_recv()
    for r in range(1, tpn):
        t = flipped(me_t, r, tpn)
        group_copy(t, 0, row_count).wait_recv()

    part = min(row_count, 32)
    for first in range(0, row_count, part):
        v = wide[first : first + part, :].astype(f32)
        average = jnp.sum(v, axis=1, keepdims=True) / full
        spread = jnp.sum(v * v, axis=1, keepdims=True) / full - average * average
        v = (v - average) * lax.rsqrt(spread + EPSILON) * gains[0:1, :] + gains[1:2, :]
        v = v / (1.0 + jnp.exp(-v))
        energy = jnp.sum(v * v, axis=1, keepdims=True) / full
        branch[first : first + part, :] = (v * lax.rsqrt(energy + EPSILON) * gains[2:3, :]).astype(bf)

    tile = min(hidden, 512)
    inner = (me_z > 0) & (me_z < spn - 1)

    def project(c, carry):
        cols = pl.ds(pl.multiple_of(c * tile, tile), tile)
        h = residual[:, cols].astype(f32) + jnp.dot(
            branch[...], w_out[:, cols], preferred_element_type=f32
        )
        h = h.astype(bf)
        hid[:, cols] = h
        picked = jnp.dot(pick[...], h, preferred_element_type=f32).astype(bf)
        for k in range(pieces):
            at = COLUMNS.index(k) * height
            taken = picked[at : at + height]
            if k < SPLIT:
                rows[k, 0, :, cols] = taken
            else:
                send[k, :, cols] = taken
        x_copy(0, cols).start()

        @pl.when(inner)
        def _():
            for k in INNER[:INNER_PARTS]:
                z_copy(k, cols).start()

        @pl.when(jnp.logical_not(inner))
        def _():
            for k in OUTER[:OUTER_PARTS]:
                z_copy(k, cols).start()

        return carry

    lax.fori_loop(0, width // tile, project, 0)
    pair_copy(0).start()

    @pl.when(inner)
    def _():
        for k in INNER[INNER_PARTS:]:
            z_copy(k).start()

    @pl.when(jnp.logical_not(inner))
    def _():
        for k in OUTER[OUTER_PARTS:]:
            z_copy(k).start()


    row_of, lane_of = (lax.broadcasted_iota(jnp.int32, (height, LANES), d) for d in (0, 1))

    def compute(k):
        strip = height // 2
        for r in range(tpn):
            for first in range(0, height, strip):
                h = rows[k, r, first : first + strip].astype(f32)
                level = lax.rsqrt(jnp.sum(h * h, axis=1, keepdims=True) / width + EPSILON)
                low = r * height + first
                normed[low : low + strip] = (h * level * moe_gain[...]).astype(bf)
        x = normed[...]
        diagonal = lane_of == row_of + (k % SPLIT) * height
        for c in range(0, hidden, 256):
            g = jnp.dot(x, w_gate[:, c : c + 256], preferred_element_type=jnp.float32)
            u = jnp.dot(x, w_up[:, c : c + 256], preferred_element_type=jnp.float32)
            act[:, c : c + 256] = (g / (1.0 + jnp.exp(-g)) * u).astype(jnp.bfloat16)
        a = act[...]
        scales = [
            jnp.sum(jnp.where(diagonal, weights[k // SPLIT, r, pl.ds(me_t, 1), :], 0.0), axis=1, keepdims=True)
            for r in range(tpn)
        ]

        def column(c, carry):
            cols = pl.ds(pl.multiple_of(c * tile, tile), tile)
            res = jnp.dot(a, w_down[:, cols], preferred_element_type=jnp.float32).astype(jnp.bfloat16)
            res = res.astype(jnp.float32)
            parts = [res[r * height : (r + 1) * height] * scales[r] for r in range(tpn)]
            half_out[k, 0, :, cols] = parts[1].astype(jnp.bfloat16)
            half_out[k, 1, :, cols] = parts[3].astype(jnp.bfloat16)
            own[k, 0, :, cols] = parts[0]
            own[k, 1, :, cols] = parts[2]
            return carry

        lax.fori_loop(0, width // tile, column, 0)

    def first(k):
        x_copy(k).start()
        pair_copy(k).start()

    def forward(k):
        z_copy(k).wait_recv()
        first(k)

    def relay(k):
        x_copy(k).wait_recv()
        via_copy(k).start()

    def run(k):
        pair_copy(k).wait_recv()
        via_copy(k).wait_recv()
        compute(k)
        half_copy(k).start()

    def halve(k):
        half_copy(k).wait_recv()
        cross_out[k] = (own[k, 1] + half_in[k, 1].astype(jnp.float32)).astype(jnp.bfloat16)

    def cross(k):
        cross_copy(k).start()

    def finish(k):
        cross_copy(k).wait_recv()
        ready = (
            own[k, 0] + half_in[k, 0].astype(jnp.float32) + cross_in[k].astype(jnp.float32)
        ).astype(jnp.bfloat16)
        if k < SPLIT:
            back[COLUMNS.index(k)] = ready
        else:
            final[k] = ready
            back_copy(k).start()

    def arrive(k):
        for q, r in peers:
            meta_copy(q, r).wait_recv()
        for load in loads[1:]:
            load.wait()

    acts = {"m": arrive, "f": first, "z": forward, "x": relay, "c": run, "h": halve, "b": cross, "e": finish}
    for line in PLAN:
        for word in line.split():
            acts[word[0]](int(word[1:]))

    edge = LATE * height
    for k in COLUMNS[LATE:]:
        if k >= SPLIT:
            back_copy(k).wait_recv()
    for c in range(0, width, tile):
        moved = back[LATE:, :, c : c + tile].reshape((pieces - LATE) * height, tile)
        total[:, c : c + tile] = hid[:, c : c + tile].astype(f32) + jnp.dot(
            unpick[:, edge:], moved, preferred_element_type=f32
        )
    for k in COLUMNS[:LATE]:
        if k >= SPLIT:
            back_copy(k).wait_recv()

    for c in range(0, width, tile):
        moved = back[:LATE, :, c : c + tile].reshape(edge, tile)
        result[:, c : c + tile] = (
            total[:, c : c + tile] + jnp.dot(unpick[:, :edge], moved, preferred_element_type=f32)
        ).astype(bf)

    @pl.when(me_z < spn - 1)
    def _():
        halo_copy(me_z + 1).wait_send()

    for r in range(1, tpn):
        gain_copy(r).wait_send()
        group_copy(flipped(me_t, r, tpn), 0, row_count).wait_send()
    for q, r in peers:
        meta_copy(q, r).wait_send()
    for k in range(pieces):
        for make in (x_copy, pair_copy, via_copy, half_copy, cross_copy):
            make(k).wait_send()
    for k in range(SPLIT, pieces):
        z_copy(k).wait_send()
        back_copy(k).wait_send()


def fused_layer(
    conv_value,
    conv_gate,
    kernel,
    conv_bias,
    ln_gain,
    ln_bias,
    out_gain,
    out_weight,
    residual,
    moe_gain,
    expert_ids,
    expert_weights,
    w_gate,
    w_up,
    w_down,
):
    spn, tpn = lax.axis_size("sp"), lax.axis_size("tp")
    tok_rows, channels = conv_value.shape
    row_count, width = residual.shape
    hidden = w_gate.shape[2]
    capacity = 2 * row_count // min(row_count, spn * tpn // 2)
    cap = tpn * capacity // 2
    pieces, height = spn * SPLIT, cap // SPLIT
    reach = -(-(kernel.shape[0] - 1) // SUBLANES) * SUBLANES
    bf, f32, dma = jnp.bfloat16, jnp.float32, pltpu.SemaphoreType.DMA
    hbm = pl.BlockSpec(memory_space=pl.ANY)
    return pl.pallas_call(
        layer_kernel,
        out_shape=pltpu.VMEM((row_count, width), bf),
        in_specs=[hbm] * 15,
        out_specs=pl.BlockSpec(memory_space=pltpu.VMEM),
        scratch_shapes=[
            pltpu.VMEM(conv_value.shape, bf),
            pltpu.VMEM(conv_gate.shape, bf),
            pltpu.VMEM(kernel.shape, bf),
            pltpu.VMEM((4, channels), f32),
            pltpu.VMEM(residual.shape, bf),
            pltpu.VMEM((1, width), f32),
            pltpu.VMEM((2, row_count), jnp.int32),
            pltpu.VMEM((2, row_count), f32),
            pltpu.VMEM(out_weight.shape, bf),
            pltpu.VMEM(w_gate.shape[1:], bf),
            pltpu.VMEM(w_up.shape[1:], bf),
            pltpu.VMEM(w_down.shape[1:], bf),
            pltpu.VMEM((reach + SUBLANES, channels), f32),
            pltpu.VMEM((spn, SUBLANES, LANES), f32),
            pltpu.VMEM((spn * cap, row_count), bf),
            pltpu.VMEM((row_count, spn * cap), bf),
            pltpu.VMEM((reach + tok_rows, channels), f32),
            pltpu.VMEM((reach, channels), bf),
            pltpu.VMEM((reach, channels), bf),
            pltpu.VMEM((tpn, row_count, channels), bf),
            pltpu.VMEM((row_count, channels * tpn), bf),
            pltpu.VMEM((4, channels * tpn), f32),
            pltpu.VMEM((row_count, channels * tpn), bf),
            pltpu.VMEM((row_count, width), bf),
            pltpu.VMEM((pieces, height, width), bf),
            pltpu.VMEM((pieces, height, width), bf),
            pltpu.VMEM((pieces, tpn, height, width), bf),
            pltpu.VMEM((tpn * height, width), bf),
            pltpu.VMEM((spn, tpn, SUBLANES, LANES), f32),
            pltpu.VMEM((pieces, 2, height, width), f32),
            pltpu.VMEM((pieces, 2, height, width), bf),
            pltpu.VMEM((pieces, 2, height, width), bf),
            pltpu.VMEM((pieces, height, width), bf),
            pltpu.VMEM((pieces, height, width), bf),
            pltpu.VMEM((pieces, height, width), bf),
            pltpu.VMEM((tpn * height, hidden), bf),
            pltpu.VMEM((row_count, width), f32),
            dma((4,)),
            dma((11,)),
            dma((spn, tpn)),
            dma((spn, tpn)),
            dma((1,)),
            dma((1,)),
        ]
        + [dma((tpn,))] * 4
        + [dma((pieces,))] * 14,
        compiler_params=pltpu.CompilerParams(collective_id=0, has_side_effects=True),
    )(
        conv_value, conv_gate, kernel, conv_bias[None, :], ln_gain[None, :], ln_bias[None, :],
        out_gain[None, :], residual, moe_gain[None, :], expert_ids.T, expert_weights.T,
        out_weight, w_gate[0], w_up[0], w_down[0],
    )


def passed_along(block, axis, distance):
    devices = range(lax.axis_size(axis))
    route = [(i - distance, i) for i in devices if i - distance in devices]
    return lax.ppermute(block, axis, route)


def per_device(
    conv_value,
    conv_gate,
    kernel,
    conv_bias,
    ln_gain,
    ln_bias,
    out_gain,
    out_weight,
    residual,
    moe_gain,
    expert_ids,
    expert_weights,
    w_gate,
    w_up,
    w_down,
):
    tpn = lax.axis_size("tp")
    if lax.axis_size("sp") == GROUPS and tpn == 4:
        return fused_layer(
            conv_value, conv_gate, kernel, conv_bias, ln_gain, ln_bias, out_gain, out_weight, residual,
            moe_gain, expert_ids, expert_weights, w_gate, w_up, w_down,
        )
    tok_rows, channels = conv_value.shape
    reach_rows = kernel.shape[0] - 1
    full_channels = channels * lax.axis_size("tp")
    gated = (conv_value.astype(jnp.float32) * jax.nn.sigmoid(conv_gate.astype(jnp.float32))).astype(
        jnp.bfloat16
    )
    before = passed_along(gated[tok_rows - reach_rows :], "sp", 1)
    padded = jnp.concatenate([before, gated], axis=0)
    convolved = jnp.zeros((tok_rows, channels), jnp.float32) + conv_bias
    for offset in range(reach_rows + 1):
        convolved = convolved + padded[offset : offset + tok_rows].astype(jnp.float32) * kernel[
            offset
        ].astype(jnp.float32)
    totals = lax.psum((jnp.sum(convolved, axis=1), jnp.sum(convolved * convolved, axis=1)), "tp")
    average = (totals[0] / full_channels)[:, None]
    spread = (totals[1] / full_channels)[:, None] - average * average
    swished = jax.nn.silu((convolved - average) * lax.rsqrt(spread + EPSILON) * ln_gain + ln_bias)
    energy = lax.psum(jnp.sum(swished * swished, axis=1), "tp")
    branch = (swished * lax.rsqrt(energy / full_channels + EPSILON)[:, None] * out_gain).astype(
        jnp.bfloat16
    )
    row_count = tok_rows // lax.axis_size("tp")
    regrouped = lax.all_to_all(branch, "tp", split_axis=0, concat_axis=1, tiled=True)
    projected = jnp.dot(regrouped, out_weight, preferred_element_type=jnp.float32)
    hidden = (residual.astype(jnp.float32) + projected).astype(jnp.bfloat16)
    widened = hidden.astype(jnp.float32)
    normed = (
        widened * lax.rsqrt(jnp.mean(widened * widened, axis=1, keepdims=True) + EPSILON) * moe_gain
    ).astype(jnp.bfloat16)
    width = normed.shape[1]
    experts = lax.axis_size("sp") * lax.axis_size("tp")
    capacity = 2 * row_count // min(row_count, experts // 2)
    flat_ids = expert_ids.reshape(-1)
    onehot = (flat_ids[:, None] == jnp.arange(experts, dtype=jnp.int32)[None, :]).astype(jnp.int32)
    slot_rank = jnp.sum((jnp.cumsum(onehot, axis=0) - 1) * onehot, axis=1)
    position = flat_ids * capacity + slot_rank
    outgoing = (
        jnp.zeros((experts * capacity, width), jnp.bfloat16)
        .at[position]
        .set(jnp.repeat(normed, 2, axis=0))
    )
    outgoing = outgoing.reshape(experts, capacity, width)
    arriving = lax.all_to_all(outgoing, ("sp", "tp"), split_axis=0, concat_axis=0, tiled=True)
    flattened = arriving.reshape(-1, width)
    gate_part = jnp.dot(flattened, w_gate[0], preferred_element_type=jnp.float32)
    up_part = jnp.dot(flattened, w_up[0], preferred_element_type=jnp.float32)
    active = (jax.nn.silu(gate_part) * up_part).astype(jnp.bfloat16)
    result = jnp.dot(active, w_down[0], preferred_element_type=jnp.float32).astype(jnp.bfloat16)
    produced = result.reshape(arriving.shape)
    returned = lax.all_to_all(produced, ("sp", "tp"), split_axis=0, concat_axis=0, tiled=True)
    returned = returned.reshape(experts * capacity, width)
    picked = returned[position].reshape(row_count, 2, width)
    combined = jnp.sum(picked.astype(jnp.float32) * expert_weights[:, :, None], axis=1)
    return (widened + combined).astype(jnp.bfloat16)


def solution(mesh):
    in_specs = (
        P(("grp", "sp"), "tp"),
        P(("grp", "sp"), "tp"),
        P(None, "tp"),
        P("tp"),
        P("tp"),
        P("tp"),
        P("tp"),
        P(),
        P(("grp", "sp", "tp"), None),
        P(),
        P(("grp", "sp", "tp"), None),
        P(("grp", "sp", "tp"), None),
        P(("sp", "tp"), None, None),
        P(("sp", "tp"), None, None),
        P(("sp", "tp"), None, None),
    )
    out_specs = P(("grp", "sp", "tp"), None)
    return jax.shard_map(
        per_device, mesh=mesh, in_specs=in_specs, out_specs=out_specs, check_vma=False
    )
```

```python
import jax
import jax.numpy as jnp
from jax import lax
from jax.experimental import pallas as pl
from jax.experimental.pallas import tpu as pltpu
from jax.sharding import PartitionSpec as P

EPSILON = 1e-06
GROUPS = 4
SPLIT = 2
LANES = 128
SUBLANES = 8
MESH = pl.DeviceIdType.MESH
COLUMNS, LATE = (2, 5, 1, 0, 3, 4, 6, 7), 4
OUTER, OUTER_PARTS = (6, 3, 4, 2, 5, 7), 1
INNER, INNER_PARTS = (3, 6, 4, 7, 2, 5), 2
PLAN = (
    "f1 z6 x0 z3",
    "m0 c0 x6 z4",
    "c6 z2 h6 b6",
    "x1 x4 c4 x3",
    "z7 c3 e6 z5",
    "h4 x2 c1 x7",
    "b4 c7 h3 h0",
    "h1 b3 x5 h7",
    "b7 e4 c2 c5",
    "h2 h5 b5 b2",
    "b1 b0 e3 e7",
    "e5 e2 e1 e0",
)


def flipped(index, mask, size):
    total, bit = 0, 1
    while bit < size:
        total = total + ((index // bit + mask // bit) % 2) * bit
        bit *= 2
    return total


def gray(index):
    return flipped(index, index // 2, 4)


def layer_kernel(
    value_hbm, gate_hbm_in, kernel_hbm, bias_hbm, lgain_hbm, lbias_hbm, ogain_hbm, res_hbm, mgain_hbm, ids_hbm, shares_hbm,
    out_hbm, gate_hbm, up_hbm, down_hbm, result,
    value, gate, kernel, params, residual, moe_gain, ids, shares,
    w_out, w_gate, w_up, w_down, taps, meta, pick, unpick, padded, halo_out, halo_in, conv, wide, gains, branch, hid,
    send, back, rows, normed, weights, own, half_out, half_in, cross_out, cross_in, final, act, total,
    low, high, load_sem, in_sem, meta_s, meta_r, halo_s, halo_r, gain_s, gain_r, group_s, group_r,
    z_s, z_r, pair_s, pair_r, x_s, x_r, via_s, via_r,
    half_s, half_r, cross_s, cross_r, back_s, back_r,
):
    spn, tpn = weights.shape[:2]
    pieces, _, height, width = rows.shape
    cap = height * SPLIT
    last = pieces - 1
    me_z, me_t = lax.axis_index("sp"), lax.axis_index("tp")
    pair, across = flipped(me_t, 1, tpn), flipped(me_t, 2, tpn)
    hidden = w_gate.shape[1]
    tok_rows, channels = value.shape
    row_count = tok_rows // tpn
    full = channels * tpn
    reach = padded.shape[0] - tok_rows
    tap_count = kernel.shape[0]
    f32, bf = jnp.float32, jnp.bfloat16

    def to(z, t):
        return {"sp": z, "tp": t}

    def copy(src, dst, s, r, z, t):
        return pltpu.make_async_remote_copy(
            src_ref=src, dst_ref=dst, send_sem=s, recv_sem=r, device_id=to(z, t), device_id_type=MESH
        )

    peers = [(q, r) for q in range(spn) for r in range(tpn) if q or r]
    below, above = me_z > 0, me_z < spn - 1
    barrier = pltpu.get_barrier_semaphore()

    def tell(semaphore, z, t):
        pl.semaphore_signal(semaphore, inc=1, device_id=to(z, t), device_id_type=MESH)

    for r in range(1, tpn):
        tell(barrier, me_z, flipped(me_t, r, tpn))

    @pl.when(below)
    def _():
        tell(barrier, me_z - 1, me_t)

    @pl.when(above)
    def _():
        tell(barrier, me_z + 1, me_t)

    def pass_on(d):
        @pl.when(me_z >= d)
        def _():
            pl.semaphore_wait(low.at[d], 1)

            @pl.when(above)
            def _():
                tell(low.at[d + 1], me_z + 1, me_t)

        @pl.when(me_z + d < spn)
        def _():
            pl.semaphore_wait(high.at[d], 1)

            @pl.when(below)
            def _():
                tell(high.at[d + 1], me_z - 1, me_t)

    inputs = [
        pltpu.make_async_copy(a, b, in_sem.at[i])
        for i, (a, b) in enumerate((
            (value_hbm, value), (gate_hbm_in, gate), (kernel_hbm, kernel), (bias_hbm, params.at[pl.ds(3, 1)]),
            (lgain_hbm, params.at[pl.ds(0, 1)]), (lbias_hbm, params.at[pl.ds(1, 1)]),
            (ogain_hbm, params.at[pl.ds(2, 1)]), (ids_hbm, ids), (shares_hbm, shares),
            (res_hbm, residual), (mgain_hbm, moe_gain),
        ))
    ]
    loads = [
        pltpu.make_async_copy(a, b, load_sem.at[i])
        for i, (a, b) in enumerate(((out_hbm, w_out), (gate_hbm, w_gate), (up_hbm, w_up), (down_hbm, w_down)))
    ]
    for load in inputs + loads:
        load.start()

    for load in inputs[:7]:
        load.wait()
    taps[:tap_count, :] = kernel[...].astype(f32)
    gated = (value[...].astype(f32) / (1.0 + jnp.exp(-gate[...].astype(f32)))).astype(bf)
    padded[reach:, :] = gated.astype(f32)
    halo_out[...] = gated[tok_rows - reach :]

    mine = pl.ds(pl.multiple_of(me_t * channels, channels), channels)

    def halo_copy(z):
        return copy(halo_out, halo_in, halo_s.at[0], halo_r.at[0], z, me_t)

    def gain_copy(r):
        return copy(params, gains.at[:, mine], gain_s.at[r], gain_r.at[r], me_z, flipped(me_t, r, tpn))

    def group_copy(t, low, high):
        span = pl.ds(low, high - low)
        r = flipped(me_t, t, tpn)
        return copy(conv.at[t, span], wide.at[span, mine], group_s.at[r], group_r.at[r], me_z, t)

    def z_copy(k, cols=pl.ds(0, width)):
        return copy(
            send.at[k, :, cols], rows.at[k, 0, :, cols], z_s.at[k], z_r.at[k],
            flipped(me_z, gray(k // SPLIT), spn), me_t,
        )

    def meta_copy(q, r):
        return copy(
            meta.at[q], weights.at[q, r], meta_s.at[q, r], meta_r.at[q, r],
            flipped(me_z, gray(q), spn), flipped(me_t, r, tpn),
        )

    def pair_copy(k):
        return copy(rows.at[k, 0], rows.at[k, 1], pair_s.at[k], pair_r.at[k], me_z, pair)

    def x_copy(k, cols=pl.ds(0, width)):
        return copy(
            rows.at[k, 0, :, cols], rows.at[k, 2, :, cols], x_s.at[k], x_r.at[k], me_z, across
        )

    def via_copy(k):
        return copy(rows.at[k, 2], rows.at[k, 3], via_s.at[k], via_r.at[k], me_z, pair)

    def half_copy(k):
        return copy(half_out.at[k], half_in.at[k], half_s.at[k], half_r.at[k], me_z, pair)

    def cross_copy(k):
        return copy(cross_out.at[k], cross_in.at[k], cross_s.at[k], cross_r.at[k], me_z, across)

    def back_copy(k):
        return copy(
            final.at[k], back.at[COLUMNS.index(k)], back_s.at[k], back_r.at[k], flipped(me_z, gray(k // SPLIT), spn), me_t
        )

    def convolve(block, first, count):
        start = pl.multiple_of(block * row_count + first, SUBLANES)
        for c in range(0, channels, LANES):
            window = padded[pl.ds(start, count + reach), c : c + LANES]
            sums = jnp.zeros((count, LANES), f32) + params[3:4, c : c + LANES]
            for b in range(SUBLANES):
                extent = count + (SUBLANES if b else 0)
                group = None
                for a in range(0, reach + 1, SUBLANES):
                    tap = a + b - (reach - tap_count + 1)
                    if 0 <= tap < tap_count:
                        term = window[a : a + extent] * taps[tap : tap + 1, c : c + LANES]
                        group = term if group is None else group + term
                sums = sums + group[b : b + count]
            conv[block, first : first + count, c : c + LANES] = sums.astype(bf)

    side = me_t // 2
    for j, b in enumerate((2, 3, 1, 0)):
        block = b + side * (3 - 2 * b)
        edge = b in (0, 3)
        convolve(block, reach, row_count - reach)
        if edge:
            @pl.when(block != 0)
            def _():
                convolve(block, 0, reach)
        else:
            convolve(block, 0, reach)
        if j == 0:
            pl.semaphore_wait(barrier, tpn - 1 + jnp.where(below & above, 2, 1))

            @pl.when(above)
            def _():
                halo_copy(me_z + 1).start()
                tell(low.at[1], me_z + 1, me_t)

            @pl.when(below)
            def _():
                tell(high.at[1], me_z - 1, me_t)

            for r in range(1, tpn):
                gain_copy(r).start()

        if edge:
            @pl.when((block != me_t) & (block != 0))
            def _():
                group_copy(block, 0, row_count).start()

            @pl.when((block != me_t) & (block == 0))
            def _():
                group_copy(block, reach, row_count).start()
        else:
            @pl.when(block != me_t)
            def _():
                group_copy(block, 0, row_count).start()

    @pl.when(me_z == 0)
    def _():
        padded[:reach, :] = jnp.zeros((reach, channels), f32)

    @pl.when(me_z > 0)
    def _():
        halo_copy(me_z - 1).wait_recv()
        padded[:reach, :] = halo_in[...].astype(f32)

    convolve(0, 0, reach)

    @pl.when(me_t != 0)
    def _():
        group_copy(0, 0, reach).start()

    wide[:, mine] = conv[me_t]
    gains[:, mine] = params[...]

    pass_on(1)
    for load in inputs[7:9]:
        load.wait()
    square = (row_count, row_count)
    down, along = (lax.broadcasted_iota(jnp.int32, square, d) for d in (0, 1))

    def upright(line):
        return jnp.sum(
            jnp.where(down == along, jnp.broadcast_to(line, square), jnp.zeros((), line.dtype)),
            axis=1, keepdims=True,
        )

    def distance(number):
        mask = jnp.bitwise_xor(number, me_z)
        return jnp.bitwise_xor(mask, lax.div(mask, 2))

    def place(number, order):
        found = distance(number) * SPLIT + lax.div(order, height)
        column = sum(jnp.where(found == k, c, 0) for c, k in enumerate(COLUMNS))
        return column * height + lax.rem(order, height)

    group_row = jnp.broadcast_to(lax.div(ids[0:1, :], tpn), square)
    group = jnp.broadcast_to(upright(group_row[0:1, :]), square)
    same = group == group_row
    rank = jnp.sum(jnp.where(same & (along < down), 1, 0), axis=1, keepdims=True)
    rank_row = jnp.sum(jnp.where(same & (down < along), 1, 0), axis=0, keepdims=True)
    slot = place(group[:, 0:1], rank)
    slot_row = place(group_row[0:1, :], rank_row)
    slots = spn * cap
    pick[...] = jnp.where(
        lax.broadcasted_iota(jnp.int32, (slots, row_count), 0) == slot_row, 1.0, 0.0
    ).astype(bf)
    unpick[...] = jnp.where(
        lax.broadcasted_iota(jnp.int32, (row_count, slots), 1) == slot, 1.0, 0.0
    ).astype(bf)
    lane = lax.broadcasted_iota(jnp.int32, (row_count, LANES), 1)
    experts = lax.rem(ids[...], tpn)
    meta[...] = jnp.zeros_like(meta)
    by_expert = [
        upright(jnp.sum(jnp.where(experts == e, shares[...], 0.0), axis=0, keepdims=True))
        for e in range(tpn)
    ]
    for q in range(spn):
        here = (distance(group[:, 0:1]) == q) & (lane == rank)
        for e in range(tpn):
            share = by_expert[e]
            meta[q, e : e + 1, :] = jnp.sum(jnp.where(here, share, 0.0), axis=0, keepdims=True)
    weights[0, 0] = meta[0]
    for d in range(2, spn):
        pass_on(d)
    for q, r in peers:
        meta_copy(q, r).start()

    for load in inputs[9:]:
        load.wait()
    loads[0].wait()
    for r in range(1, tpn):
        gain_copy(r).wait_recv()
    for r in range(1, tpn):
        t = flipped(me_t, r, tpn)
        group_copy(t, 0, row_count).wait_recv()

    part = min(row_count, 32)
    for first in range(0, row_count, part):
        v = wide[first : first + part, :].astype(f32)
        average = jnp.sum(v, axis=1, keepdims=True) / full
        spread = jnp.sum(v * v, axis=1, keepdims=True) / full - average * average
        v = (v - average) * lax.rsqrt(spread + EPSILON) * gains[0:1, :] + gains[1:2, :]
        v = v / (1.0 + jnp.exp(-v))
        energy = jnp.sum(v * v, axis=1, keepdims=True) / full
        branch[first : first + part, :] = (v * lax.rsqrt(energy + EPSILON) * gains[2:3, :]).astype(bf)

    tile = min(hidden, 512)
    inner = (me_z > 0) & (me_z < spn - 1)

    def project(c, carry):
        cols = pl.ds(pl.multiple_of(c * tile, tile), tile)
        h = residual[:, cols].astype(f32) + jnp.dot(
            branch[...], w_out[:, cols], preferred_element_type=f32
        )
        h = h.astype(bf)
        hid[:, cols] = h
        picked = jnp.dot(pick[...], h, preferred_element_type=f32).astype(bf)
        for k in range(pieces):
            at = COLUMNS.index(k) * height
            taken = picked[at : at + height]
            if k < SPLIT:
                rows[k, 0, :, cols] = taken
            else:
                send[k, :, cols] = taken
        x_copy(0, cols).start()

        @pl.when(inner)
        def _():
            for k in INNER[:INNER_PARTS]:
                z_copy(k, cols).start()

        @pl.when(jnp.logical_not(inner))
        def _():
            for k in OUTER[:OUTER_PARTS]:
                z_copy(k, cols).start()

        return carry

    lax.fori_loop(0, width // tile, project, 0)
    pair_copy(0).start()

    @pl.when(inner)
    def _():
        for k in INNER[INNER_PARTS:]:
            z_copy(k).start()

    @pl.when(jnp.logical_not(inner))
    def _():
        for k in OUTER[OUTER_PARTS:]:
            z_copy(k).start()


    row_of, lane_of = (lax.broadcasted_iota(jnp.int32, (height, LANES), d) for d in (0, 1))

    def compute(k):
        strip = height // 2
        for r in range(tpn):
            for first in range(0, height, strip):
                h = rows[k, r, first : first + strip].astype(f32)
                level = lax.rsqrt(jnp.sum(h * h, axis=1, keepdims=True) / width + EPSILON)
                low = r * height + first
                normed[low : low + strip] = (h * level * moe_gain[...]).astype(bf)
        x = normed[...]
        diagonal = lane_of == row_of + (k % SPLIT) * height
        for c in range(0, hidden, 256):
            g = jnp.dot(x, w_gate[:, c : c + 256], preferred_element_type=jnp.float32)
            u = jnp.dot(x, w_up[:, c : c + 256], preferred_element_type=jnp.float32)
            act[:, c : c + 256] = (g / (1.0 + jnp.exp(-g)) * u).astype(jnp.bfloat16)
        a = act[...]
        scales = [
            jnp.sum(jnp.where(diagonal, weights[k // SPLIT, r, pl.ds(me_t, 1), :], 0.0), axis=1, keepdims=True)
            for r in range(tpn)
        ]

        def column(c, carry):
            cols = pl.ds(pl.multiple_of(c * tile, tile), tile)
            res = jnp.dot(a, w_down[:, cols], preferred_element_type=jnp.float32).astype(jnp.bfloat16)
            res = res.astype(jnp.float32)
            parts = [res[r * height : (r + 1) * height] * scales[r] for r in range(tpn)]
            half_out[k, 0, :, cols] = parts[1].astype(jnp.bfloat16)
            half_out[k, 1, :, cols] = parts[3].astype(jnp.bfloat16)
            own[k, 0, :, cols] = parts[0]
            own[k, 1, :, cols] = parts[2]
            return carry

        lax.fori_loop(0, width // tile, column, 0)

    def first(k):
        x_copy(k).start()
        pair_copy(k).start()

    def forward(k):
        z_copy(k).wait_recv()
        first(k)

    def relay(k):
        x_copy(k).wait_recv()
        via_copy(k).start()

    def run(k):
        pair_copy(k).wait_recv()
        via_copy(k).wait_recv()
        compute(k)
        half_copy(k).start()

    def halve(k):
        half_copy(k).wait_recv()
        cross_out[k] = (own[k, 1] + half_in[k, 1].astype(jnp.float32)).astype(jnp.bfloat16)

    def cross(k):
        cross_copy(k).start()

    def finish(k):
        cross_copy(k).wait_recv()
        ready = (
            own[k, 0] + half_in[k, 0].astype(jnp.float32) + cross_in[k].astype(jnp.float32)
        ).astype(jnp.bfloat16)
        if k < SPLIT:
            back[COLUMNS.index(k)] = ready
        else:
            final[k] = ready
            back_copy(k).start()

    def arrive(k):
        for q, r in peers:
            meta_copy(q, r).wait_recv()
        for load in loads[1:]:
            load.wait()

    acts = {"m": arrive, "f": first, "z": forward, "x": relay, "c": run, "h": halve, "b": cross, "e": finish}
    for line in PLAN:
        for word in line.split():
            acts[word[0]](int(word[1:]))

    edge = LATE * height
    for k in COLUMNS[LATE:]:
        if k >= SPLIT:
            back_copy(k).wait_recv()
    for c in range(0, width, tile):
        moved = back[LATE:, :, c : c + tile].reshape((pieces - LATE) * height, tile)
        total[:, c : c + tile] = hid[:, c : c + tile].astype(f32) + jnp.dot(
            unpick[:, edge:], moved, preferred_element_type=f32
        )
    for k in COLUMNS[:LATE]:
        if k >= SPLIT:
            back_copy(k).wait_recv()

    for c in range(0, width, tile):
        moved = back[:LATE, :, c : c + tile].reshape(edge, tile)
        result[:, c : c + tile] = (
            total[:, c : c + tile] + jnp.dot(unpick[:, :edge], moved, preferred_element_type=f32)
        ).astype(bf)

    @pl.when(me_z < spn - 1)
    def _():
        halo_copy(me_z + 1).wait_send()

    for r in range(1, tpn):
        gain_copy(r).wait_send()
        group_copy(flipped(me_t, r, tpn), 0, row_count).wait_send()
    for q, r in peers:
        meta_copy(q, r).wait_send()
    for k in range(pieces):
        for make in (x_copy, pair_copy, via_copy, half_copy, cross_copy):
            make(k).wait_send()
    for k in range(SPLIT, pieces):
        z_copy(k).wait_send()
        back_copy(k).wait_send()


def fused_layer(
    conv_value,
    conv_gate,
    kernel,
    conv_bias,
    ln_gain,
    ln_bias,
    out_gain,
    out_weight,
    residual,
    moe_gain,
    expert_ids,
    expert_weights,
    w_gate,
    w_up,
    w_down,
):
    spn, tpn = lax.axis_size("sp"), lax.axis_size("tp")
    tok_rows, channels = conv_value.shape
    row_count, width = residual.shape
    hidden = w_gate.shape[2]
    capacity = 2 * row_count // min(row_count, spn * tpn // 2)
    cap = tpn * capacity // 2
    pieces, height = spn * SPLIT, cap // SPLIT
    reach = -(-(kernel.shape[0] - 1) // SUBLANES) * SUBLANES
    bf, f32, dma = jnp.bfloat16, jnp.float32, pltpu.SemaphoreType.DMA
    hbm = pl.BlockSpec(memory_space=pl.ANY)
    return pl.pallas_call(
        layer_kernel,
        out_shape=pltpu.VMEM((row_count, width), bf),
        in_specs=[hbm] * 15,
        out_specs=pl.BlockSpec(memory_space=pltpu.VMEM),
        scratch_shapes=[
            pltpu.VMEM(conv_value.shape, bf),
            pltpu.VMEM(conv_gate.shape, bf),
            pltpu.VMEM(kernel.shape, bf),
            pltpu.VMEM((4, channels), f32),
            pltpu.VMEM(residual.shape, bf),
            pltpu.VMEM((1, width), f32),
            pltpu.VMEM((2, row_count), jnp.int32),
            pltpu.VMEM((2, row_count), f32),
            pltpu.VMEM(out_weight.shape, bf),
            pltpu.VMEM(w_gate.shape[1:], bf),
            pltpu.VMEM(w_up.shape[1:], bf),
            pltpu.VMEM(w_down.shape[1:], bf),
            pltpu.VMEM((reach + SUBLANES, channels), f32),
            pltpu.VMEM((spn, SUBLANES, LANES), f32),
            pltpu.VMEM((spn * cap, row_count), bf),
            pltpu.VMEM((row_count, spn * cap), bf),
            pltpu.VMEM((reach + tok_rows, channels), f32),
            pltpu.VMEM((reach, channels), bf),
            pltpu.VMEM((reach, channels), bf),
            pltpu.VMEM((tpn, row_count, channels), bf),
            pltpu.VMEM((row_count, channels * tpn), bf),
            pltpu.VMEM((4, channels * tpn), f32),
            pltpu.VMEM((row_count, channels * tpn), bf),
            pltpu.VMEM((row_count, width), bf),
            pltpu.VMEM((pieces, height, width), bf),
            pltpu.VMEM((pieces, height, width), bf),
            pltpu.VMEM((pieces, tpn, height, width), bf),
            pltpu.VMEM((tpn * height, width), bf),
            pltpu.VMEM((spn, tpn, SUBLANES, LANES), f32),
            pltpu.VMEM((pieces, 2, height, width), f32),
            pltpu.VMEM((pieces, 2, height, width), bf),
            pltpu.VMEM((pieces, 2, height, width), bf),
            pltpu.VMEM((pieces, height, width), bf),
            pltpu.VMEM((pieces, height, width), bf),
            pltpu.VMEM((pieces, height, width), bf),
            pltpu.VMEM((tpn * height, hidden), bf),
            pltpu.VMEM((row_count, width), f32),
            pltpu.SemaphoreType.REGULAR((spn + 1,)),
            pltpu.SemaphoreType.REGULAR((spn + 1,)),
            dma((4,)),
            dma((11,)),
            dma((spn, tpn)),
            dma((spn, tpn)),
            dma((1,)),
            dma((1,)),
        ]
        + [dma((tpn,))] * 4
        + [dma((pieces,))] * 14,
        compiler_params=pltpu.CompilerParams(collective_id=0, has_side_effects=True),
    )(
        conv_value, conv_gate, kernel, conv_bias[None, :], ln_gain[None, :], ln_bias[None, :],
        out_gain[None, :], residual, moe_gain[None, :], expert_ids.T, expert_weights.T,
        out_weight, w_gate[0], w_up[0], w_down[0],
    )


def passed_along(block, axis, distance):
    devices = range(lax.axis_size(axis))
    route = [(i - distance, i) for i in devices if i - distance in devices]
    return lax.ppermute(block, axis, route)


def per_device(
    conv_value,
    conv_gate,
    kernel,
    conv_bias,
    ln_gain,
    ln_bias,
    out_gain,
    out_weight,
    residual,
    moe_gain,
    expert_ids,
    expert_weights,
    w_gate,
    w_up,
    w_down,
):
    tpn = lax.axis_size("tp")
    if lax.axis_size("sp") == GROUPS and tpn == 4:
        return fused_layer(
            conv_value, conv_gate, kernel, conv_bias, ln_gain, ln_bias, out_gain, out_weight, residual,
            moe_gain, expert_ids, expert_weights, w_gate, w_up, w_down,
        )
    tok_rows, channels = conv_value.shape
    reach_rows = kernel.shape[0] - 1
    full_channels = channels * lax.axis_size("tp")
    gated = (conv_value.astype(jnp.float32) * jax.nn.sigmoid(conv_gate.astype(jnp.float32))).astype(
        jnp.bfloat16
    )
    before = passed_along(gated[tok_rows - reach_rows :], "sp", 1)
    padded = jnp.concatenate([before, gated], axis=0)
    convolved = jnp.zeros((tok_rows, channels), jnp.float32) + conv_bias
    for offset in range(reach_rows + 1):
        convolved = convolved + padded[offset : offset + tok_rows].astype(jnp.float32) * kernel[
            offset
        ].astype(jnp.float32)
    totals = lax.psum((jnp.sum(convolved, axis=1), jnp.sum(convolved * convolved, axis=1)), "tp")
    average = (totals[0] / full_channels)[:, None]
    spread = (totals[1] / full_channels)[:, None] - average * average
    swished = jax.nn.silu((convolved - average) * lax.rsqrt(spread + EPSILON) * ln_gain + ln_bias)
    energy = lax.psum(jnp.sum(swished * swished, axis=1), "tp")
    branch = (swished * lax.rsqrt(energy / full_channels + EPSILON)[:, None] * out_gain).astype(
        jnp.bfloat16
    )
    row_count = tok_rows // lax.axis_size("tp")
    regrouped = lax.all_to_all(branch, "tp", split_axis=0, concat_axis=1, tiled=True)
    projected = jnp.dot(regrouped, out_weight, preferred_element_type=jnp.float32)
    hidden = (residual.astype(jnp.float32) + projected).astype(jnp.bfloat16)
    widened = hidden.astype(jnp.float32)
    normed = (
        widened * lax.rsqrt(jnp.mean(widened * widened, axis=1, keepdims=True) + EPSILON) * moe_gain
    ).astype(jnp.bfloat16)
    width = normed.shape[1]
    experts = lax.axis_size("sp") * lax.axis_size("tp")
    capacity = 2 * row_count // min(row_count, experts // 2)
    flat_ids = expert_ids.reshape(-1)
    onehot = (flat_ids[:, None] == jnp.arange(experts, dtype=jnp.int32)[None, :]).astype(jnp.int32)
    slot_rank = jnp.sum((jnp.cumsum(onehot, axis=0) - 1) * onehot, axis=1)
    position = flat_ids * capacity + slot_rank
    outgoing = (
        jnp.zeros((experts * capacity, width), jnp.bfloat16)
        .at[position]
        .set(jnp.repeat(normed, 2, axis=0))
    )
    outgoing = outgoing.reshape(experts, capacity, width)
    arriving = lax.all_to_all(outgoing, ("sp", "tp"), split_axis=0, concat_axis=0, tiled=True)
    flattened = arriving.reshape(-1, width)
    gate_part = jnp.dot(flattened, w_gate[0], preferred_element_type=jnp.float32)
    up_part = jnp.dot(flattened, w_up[0], preferred_element_type=jnp.float32)
    active = (jax.nn.silu(gate_part) * up_part).astype(jnp.bfloat16)
    result = jnp.dot(active, w_down[0], preferred_element_type=jnp.float32).astype(jnp.bfloat16)
    produced = result.reshape(arriving.shape)
    returned = lax.all_to_all(produced, ("sp", "tp"), split_axis=0, concat_axis=0, tiled=True)
    returned = returned.reshape(experts * capacity, width)
    picked = returned[position].reshape(row_count, 2, width)
    combined = jnp.sum(picked.astype(jnp.float32) * expert_weights[:, :, None], axis=1)
    return (widened + combined).astype(jnp.bfloat16)


def solution(mesh):
    in_specs = (
        P(("grp", "sp"), "tp"),
        P(("grp", "sp"), "tp"),
        P(None, "tp"),
        P("tp"),
        P("tp"),
        P("tp"),
        P("tp"),
        P(),
        P(("grp", "sp", "tp"), None),
        P(),
        P(("grp", "sp", "tp"), None),
        P(("grp", "sp", "tp"), None),
        P(("sp", "tp"), None, None),
        P(("sp", "tp"), None, None),
        P(("sp", "tp"), None, None),
    )
    out_specs = P(("grp", "sp", "tp"), None)
    return jax.shard_map(
        per_device, mesh=mesh, in_specs=in_specs, out_specs=out_specs, check_vma=False
    )
```

```python
import jax
import jax.numpy as jnp
from jax import lax
from jax.experimental import pallas as pl
from jax.experimental.pallas import tpu as pltpu
from jax.sharding import PartitionSpec as P

EPSILON = 1e-06
GROUPS = 4
SPLIT = 2
LANES = 128
SUBLANES = 8
MESH = pl.DeviceIdType.MESH
COLUMNS, LATE = (2, 7, 1, 0, 3, 4, 5, 6), 4
OUTER, OUTER_PARTS = (4, 3, 2, 5, 7, 6), 1
INNER, INNER_PARTS = (4, 5, 3, 6, 7, 2), 1
PLAN = (
    "f1 x0 z4 z3",
    "m0 c0 x1 x4",
    "z2 c4 z5 c1",
    "x3 h4 x2 h1",
    "b4 c3 z6 x5",
    "c5 z7 h3 h5",
    "b5 x6 b3 h0",
    "e4 c2 c6 x7",
    "h2 h6 b6 e5",
    "c7 e3 b2 h7",
    "b7 e6 b1 b0",
    "e2 e7 e1 e0",
)


def flipped(index, mask, size):
    total, bit = 0, 1
    while bit < size:
        total = total + ((index // bit + mask // bit) % 2) * bit
        bit *= 2
    return total


def gray(index):
    return flipped(index, index // 2, 4)


def layer_kernel(
    value_hbm, gate_hbm_in, kernel_hbm, bias_hbm, lgain_hbm, lbias_hbm, ogain_hbm, res_hbm, mgain_hbm, ids_hbm, shares_hbm,
    out_hbm, gate_hbm, up_hbm, down_hbm, result,
    value, gate, kernel, params, residual, moe_gain, ids, shares,
    w_out, w_gate, w_up, w_down, taps, meta, pick, unpick, padded, halo_out, halo_in, conv, wide, gains, branch, hid,
    send, back, rows, normed, weights, own, half_out, half_in, cross_out, cross_in, final, act, total,
    low, high, load_sem, in_sem, meta_s, meta_r, halo_s, halo_r, gain_s, gain_r, group_s, group_r,
    z_s, z_r, pair_s, pair_r, x_s, x_r, via_s, via_r,
    half_s, half_r, cross_s, cross_r, back_s, back_r,
):
    spn, tpn = weights.shape[:2]
    pieces, _, height, width = rows.shape
    cap = height * SPLIT
    last = pieces - 1
    me_z, me_t = lax.axis_index("sp"), lax.axis_index("tp")
    pair, across = flipped(me_t, 1, tpn), flipped(me_t, 2, tpn)
    hidden = w_gate.shape[1]
    tok_rows, channels = value.shape
    row_count = tok_rows // tpn
    full = channels * tpn
    reach = padded.shape[0] - tok_rows
    tap_count = kernel.shape[0]
    f32, bf = jnp.float32, jnp.bfloat16

    def to(z, t):
        return {"sp": z, "tp": t}

    def copy(src, dst, s, r, z, t):
        return pltpu.make_async_remote_copy(
            src_ref=src, dst_ref=dst, send_sem=s, recv_sem=r, device_id=to(z, t), device_id_type=MESH
        )

    peers = [(q, r) for q in range(spn) for r in range(tpn) if q or r]
    below, above = me_z > 0, me_z < spn - 1
    barrier = pltpu.get_barrier_semaphore()

    def tell(semaphore, z, t):
        pl.semaphore_signal(semaphore, inc=1, device_id=to(z, t), device_id_type=MESH)

    for r in range(1, tpn):
        tell(barrier, me_z, flipped(me_t, r, tpn))

    @pl.when(below)
    def _():
        tell(barrier, me_z - 1, me_t)

    @pl.when(above)
    def _():
        tell(barrier, me_z + 1, me_t)

    def pass_on(d):
        @pl.when(me_z >= d)
        def _():
            pl.semaphore_wait(low.at[d], 1)

            @pl.when(above)
            def _():
                tell(low.at[d + 1], me_z + 1, me_t)

        @pl.when(me_z + d < spn)
        def _():
            pl.semaphore_wait(high.at[d], 1)

            @pl.when(below)
            def _():
                tell(high.at[d + 1], me_z - 1, me_t)

    inputs = [
        pltpu.make_async_copy(a, b, in_sem.at[i])
        for i, (a, b) in enumerate((
            (value_hbm, value), (gate_hbm_in, gate), (kernel_hbm, kernel), (bias_hbm, params.at[pl.ds(3, 1)]),
            (lgain_hbm, params.at[pl.ds(0, 1)]), (lbias_hbm, params.at[pl.ds(1, 1)]),
            (ogain_hbm, params.at[pl.ds(2, 1)]), (ids_hbm, ids), (shares_hbm, shares),
            (res_hbm, residual), (mgain_hbm, moe_gain),
        ))
    ]
    loads = [
        pltpu.make_async_copy(a, b, load_sem.at[i])
        for i, (a, b) in enumerate(((out_hbm, w_out), (gate_hbm, w_gate), (up_hbm, w_up), (down_hbm, w_down)))
    ]
    for load in inputs + loads:
        load.start()

    for load in inputs[:7]:
        load.wait()
    taps[:tap_count, :] = kernel[...].astype(f32)
    gated = (value[...].astype(f32) / (1.0 + jnp.exp(-gate[...].astype(f32)))).astype(bf)
    padded[reach:, :] = gated.astype(f32)
    halo_out[...] = gated[tok_rows - reach :]

    mine = pl.ds(pl.multiple_of(me_t * channels, channels), channels)

    def halo_copy(z):
        return copy(halo_out, halo_in, halo_s.at[0], halo_r.at[0], z, me_t)

    def gain_copy(r):
        return copy(params, gains.at[:, mine], gain_s.at[r], gain_r.at[r], me_z, flipped(me_t, r, tpn))

    def group_copy(t, low, high):
        span = pl.ds(low, high - low)
        r = flipped(me_t, t, tpn)
        return copy(conv.at[t, span], wide.at[span, mine], group_s.at[r], group_r.at[r], me_z, t)

    def z_copy(k, cols=pl.ds(0, width)):
        return copy(
            send.at[k, :, cols], rows.at[k, 0, :, cols], z_s.at[k], z_r.at[k],
            flipped(me_z, gray(k // SPLIT), spn), me_t,
        )

    def meta_copy(q, r):
        return copy(
            meta.at[q], weights.at[q, r], meta_s.at[q, r], meta_r.at[q, r],
            flipped(me_z, gray(q), spn), flipped(me_t, r, tpn),
        )

    def pair_copy(k):
        return copy(rows.at[k, 0], rows.at[k, 1], pair_s.at[k], pair_r.at[k], me_z, pair)

    def x_copy(k, cols=pl.ds(0, width)):
        return copy(
            rows.at[k, 0, :, cols], rows.at[k, 2, :, cols], x_s.at[k], x_r.at[k], me_z, across
        )

    def via_copy(k):
        return copy(rows.at[k, 2], rows.at[k, 3], via_s.at[k], via_r.at[k], me_z, pair)

    def half_copy(k):
        return copy(half_out.at[k], half_in.at[k], half_s.at[k], half_r.at[k], me_z, pair)

    def cross_copy(k):
        return copy(cross_out.at[k], cross_in.at[k], cross_s.at[k], cross_r.at[k], me_z, across)

    def back_copy(k):
        return copy(
            final.at[k], back.at[COLUMNS.index(k)], back_s.at[k], back_r.at[k], flipped(me_z, gray(k // SPLIT), spn), me_t
        )

    def convolve(block, first, count):
        start = pl.multiple_of(block * row_count + first, SUBLANES)
        for c in range(0, channels, LANES):
            window = padded[pl.ds(start, count + reach), c : c + LANES]
            sums = jnp.zeros((count, LANES), f32) + params[3:4, c : c + LANES]
            for b in range(SUBLANES):
                extent = count + (SUBLANES if b else 0)
                group = None
                for a in range(0, reach + 1, SUBLANES):
                    tap = a + b - (reach - tap_count + 1)
                    if 0 <= tap < tap_count:
                        term = window[a : a + extent] * taps[tap : tap + 1, c : c + LANES]
                        group = term if group is None else group + term
                sums = sums + group[b : b + count]
            conv[block, first : first + count, c : c + LANES] = sums.astype(bf)

    side = me_t // 2
    for j, b in enumerate((2, 3, 1, 0)):
        block = b + side * (3 - 2 * b)
        edge = b in (0, 3)
        convolve(block, reach, row_count - reach)
        if edge:
            @pl.when(block != 0)
            def _():
                convolve(block, 0, reach)
        else:
            convolve(block, 0, reach)
        if j == 0:
            pl.semaphore_wait(barrier, tpn - 1 + jnp.where(below & above, 2, 1))

            @pl.when(above)
            def _():
                halo_copy(me_z + 1).start()
                tell(low.at[1], me_z + 1, me_t)

            @pl.when(below)
            def _():
                tell(high.at[1], me_z - 1, me_t)

            for r in range(1, tpn):
                gain_copy(r).start()

        if edge:
            @pl.when((block != me_t) & (block != 0))
            def _():
                group_copy(block, 0, row_count).start()

            @pl.when((block != me_t) & (block == 0))
            def _():
                group_copy(block, reach, row_count).start()
        else:
            @pl.when(block != me_t)
            def _():
                group_copy(block, 0, row_count).start()

    @pl.when(me_z == 0)
    def _():
        padded[:reach, :] = jnp.zeros((reach, channels), f32)

    @pl.when(me_z > 0)
    def _():
        halo_copy(me_z - 1).wait_recv()
        padded[:reach, :] = halo_in[...].astype(f32)

    convolve(0, 0, reach)

    @pl.when(me_t != 0)
    def _():
        group_copy(0, 0, reach).start()

    wide[:, mine] = conv[me_t]
    gains[:, mine] = params[...]

    pass_on(1)
    for load in inputs[7:9]:
        load.wait()
    square = (row_count, row_count)
    down, along = (lax.broadcasted_iota(jnp.int32, square, d) for d in (0, 1))

    def upright(line):
        return jnp.sum(
            jnp.where(down == along, jnp.broadcast_to(line, square), jnp.zeros((), line.dtype)),
            axis=1, keepdims=True,
        )

    def distance(number):
        mask = jnp.bitwise_xor(number, me_z)
        return jnp.bitwise_xor(mask, lax.div(mask, 2))

    def place(number, order):
        found = distance(number) * SPLIT + lax.div(order, height)
        column = sum(jnp.where(found == k, c, 0) for c, k in enumerate(COLUMNS))
        return column * height + lax.rem(order, height)

    group_row = jnp.broadcast_to(lax.div(ids[0:1, :], tpn), square)
    group = jnp.broadcast_to(upright(group_row[0:1, :]), square)
    same = group == group_row
    rank = jnp.sum(jnp.where(same & (along < down), 1, 0), axis=1, keepdims=True)
    rank_row = jnp.sum(jnp.where(same & (down < along), 1, 0), axis=0, keepdims=True)
    slot = place(group[:, 0:1], rank)
    slot_row = place(group_row[0:1, :], rank_row)
    slots = spn * cap
    pick[...] = jnp.where(
        lax.broadcasted_iota(jnp.int32, (slots, row_count), 0) == slot_row, 1.0, 0.0
    ).astype(bf)
    unpick[...] = jnp.where(
        lax.broadcasted_iota(jnp.int32, (row_count, slots), 1) == slot, 1.0, 0.0
    ).astype(bf)
    lane = lax.broadcasted_iota(jnp.int32, (row_count, LANES), 1)
    experts = lax.rem(ids[...], tpn)
    meta[...] = jnp.zeros_like(meta)
    by_expert = [
        upright(jnp.sum(jnp.where(experts == e, shares[...], 0.0), axis=0, keepdims=True))
        for e in range(tpn)
    ]
    for q in range(spn):
        here = (distance(group[:, 0:1]) == q) & (lane == rank)
        for e in range(tpn):
            share = by_expert[e]
            meta[q, e : e + 1, :] = jnp.sum(jnp.where(here, share, 0.0), axis=0, keepdims=True)
    weights[0, 0] = meta[0]
    for d in range(2, spn):
        pass_on(d)
    for q, r in peers:
        meta_copy(q, r).start()

    for load in inputs[9:]:
        load.wait()
    loads[0].wait()
    for r in range(1, tpn):
        gain_copy(r).wait_recv()
    for r in range(1, tpn):
        t = flipped(me_t, r, tpn)
        group_copy(t, 0, row_count).wait_recv()

    part = min(row_count, 32)
    for first in range(0, row_count, part):
        v = wide[first : first + part, :].astype(f32)
        average = jnp.sum(v, axis=1, keepdims=True) / full
        spread = jnp.sum(v * v, axis=1, keepdims=True) / full - average * average
        v = (v - average) * lax.rsqrt(spread + EPSILON) * gains[0:1, :] + gains[1:2, :]
        v = v / (1.0 + jnp.exp(-v))
        energy = jnp.sum(v * v, axis=1, keepdims=True) / full
        branch[first : first + part, :] = (v * lax.rsqrt(energy + EPSILON) * gains[2:3, :]).astype(bf)

    tile = min(hidden, 512)
    inner = (me_z > 0) & (me_z < spn - 1)

    def project(c, carry):
        cols = pl.ds(pl.multiple_of(c * tile, tile), tile)
        h = residual[:, cols].astype(f32) + jnp.dot(
            branch[...], w_out[:, cols], preferred_element_type=f32
        )
        h = h.astype(bf)
        hid[:, cols] = h
        picked = jnp.dot(pick[...], h, preferred_element_type=f32).astype(bf)
        for k in range(pieces):
            at = COLUMNS.index(k) * height
            taken = picked[at : at + height]
            if k < SPLIT:
                rows[k, 0, :, cols] = taken
            else:
                send[k, :, cols] = taken
        x_copy(0, cols).start()

        @pl.when(inner)
        def _():
            for k in INNER[:INNER_PARTS]:
                z_copy(k, cols).start()

        @pl.when(jnp.logical_not(inner))
        def _():
            for k in OUTER[:OUTER_PARTS]:
                z_copy(k, cols).start()

        return carry

    for c in range(width // tile):
        project(c, 0)
    pair_copy(0).start()

    @pl.when(inner)
    def _():
        for k in INNER[INNER_PARTS:]:
            z_copy(k).start()

    @pl.when(jnp.logical_not(inner))
    def _():
        for k in OUTER[OUTER_PARTS:]:
            z_copy(k).start()


    row_of, lane_of = (lax.broadcasted_iota(jnp.int32, (height, LANES), d) for d in (0, 1))

    def compute(k):
        strip = height // 2
        for r in range(tpn):
            for first in range(0, height, strip):
                h = rows[k, r, first : first + strip].astype(f32)
                level = lax.rsqrt(jnp.sum(h * h, axis=1, keepdims=True) / width + EPSILON)
                low = r * height + first
                normed[low : low + strip] = (h * level * moe_gain[...]).astype(bf)
        x = normed[...]
        diagonal = lane_of == row_of + (k % SPLIT) * height
        for c in range(0, hidden, 256):
            g = jnp.dot(x, w_gate[:, c : c + 256], preferred_element_type=jnp.float32)
            u = jnp.dot(x, w_up[:, c : c + 256], preferred_element_type=jnp.float32)
            act[:, c : c + 256] = (g / (1.0 + jnp.exp(-g)) * u).astype(jnp.bfloat16)
        a = act[...]
        scales = [
            jnp.sum(jnp.where(diagonal, weights[k // SPLIT, r, pl.ds(me_t, 1), :], 0.0), axis=1, keepdims=True)
            for r in range(tpn)
        ]

        def column(c, carry):
            cols = pl.ds(pl.multiple_of(c * tile, tile), tile)
            res = jnp.dot(a, w_down[:, cols], preferred_element_type=jnp.float32).astype(jnp.bfloat16)
            res = res.astype(jnp.float32)
            parts = [res[r * height : (r + 1) * height] * scales[r] for r in range(tpn)]
            half_out[k, 0, :, cols] = parts[1].astype(jnp.bfloat16)
            half_out[k, 1, :, cols] = parts[3].astype(jnp.bfloat16)
            own[k, 0, :, cols] = parts[0]
            own[k, 1, :, cols] = parts[2]
            return carry

        lax.fori_loop(0, width // tile, column, 0)

    def first(k):
        x_copy(k).start()
        pair_copy(k).start()

    def forward(k):
        z_copy(k).wait_recv()
        first(k)

    def relay(k):
        x_copy(k).wait_recv()
        via_copy(k).start()

    def run(k):
        pair_copy(k).wait_recv()
        via_copy(k).wait_recv()
        compute(k)
        half_copy(k).start()

    def halve(k):
        half_copy(k).wait_recv()
        cross_out[k] = (own[k, 1] + half_in[k, 1].astype(jnp.float32)).astype(jnp.bfloat16)

    def cross(k):
        cross_copy(k).start()

    def finish(k):
        cross_copy(k).wait_recv()
        ready = (
            own[k, 0] + half_in[k, 0].astype(jnp.float32) + cross_in[k].astype(jnp.float32)
        ).astype(jnp.bfloat16)
        if k < SPLIT:
            back[COLUMNS.index(k)] = ready
        else:
            final[k] = ready
            back_copy(k).start()

    def arrive(k):
        for q, r in peers:
            meta_copy(q, r).wait_recv()
        for load in loads[1:]:
            load.wait()

    acts = {"m": arrive, "f": first, "z": forward, "x": relay, "c": run, "h": halve, "b": cross, "e": finish}
    for line in PLAN:
        for word in line.split():
            acts[word[0]](int(word[1:]))

    edge = LATE * height
    for k in COLUMNS[LATE:]:
        if k >= SPLIT:
            back_copy(k).wait_recv()
    for c in range(0, width, tile):
        moved = back[LATE:, :, c : c + tile].reshape((pieces - LATE) * height, tile)
        total[:, c : c + tile] = hid[:, c : c + tile].astype(f32) + jnp.dot(
            unpick[:, edge:], moved, preferred_element_type=f32
        )
    for k in COLUMNS[:LATE]:
        if k >= SPLIT:
            back_copy(k).wait_recv()

    for c in range(0, width, tile):
        moved = back[:LATE, :, c : c + tile].reshape(edge, tile)
        result[:, c : c + tile] = (
            total[:, c : c + tile] + jnp.dot(unpick[:, :edge], moved, preferred_element_type=f32)
        ).astype(bf)

    @pl.when(me_z < spn - 1)
    def _():
        halo_copy(me_z + 1).wait_send()

    for r in range(1, tpn):
        gain_copy(r).wait_send()
        group_copy(flipped(me_t, r, tpn), 0, row_count).wait_send()
    for q, r in peers:
        meta_copy(q, r).wait_send()
    for k in range(pieces):
        for make in (x_copy, pair_copy, via_copy, half_copy, cross_copy):
            make(k).wait_send()
    for k in range(SPLIT, pieces):
        z_copy(k).wait_send()
        back_copy(k).wait_send()


def fused_layer(
    conv_value,
    conv_gate,
    kernel,
    conv_bias,
    ln_gain,
    ln_bias,
    out_gain,
    out_weight,
    residual,
    moe_gain,
    expert_ids,
    expert_weights,
    w_gate,
    w_up,
    w_down,
):
    spn, tpn = lax.axis_size("sp"), lax.axis_size("tp")
    tok_rows, channels = conv_value.shape
    row_count, width = residual.shape
    hidden = w_gate.shape[2]
    capacity = 2 * row_count // min(row_count, spn * tpn // 2)
    cap = tpn * capacity // 2
    pieces, height = spn * SPLIT, cap // SPLIT
    reach = -(-(kernel.shape[0] - 1) // SUBLANES) * SUBLANES
    bf, f32, dma = jnp.bfloat16, jnp.float32, pltpu.SemaphoreType.DMA
    hbm = pl.BlockSpec(memory_space=pl.ANY)
    return pl.pallas_call(
        layer_kernel,
        out_shape=pltpu.VMEM((row_count, width), bf),
        in_specs=[hbm] * 15,
        out_specs=pl.BlockSpec(memory_space=pltpu.VMEM),
        scratch_shapes=[
            pltpu.VMEM(conv_value.shape, bf),
            pltpu.VMEM(conv_gate.shape, bf),
            pltpu.VMEM(kernel.shape, bf),
            pltpu.VMEM((4, channels), f32),
            pltpu.VMEM(residual.shape, bf),
            pltpu.VMEM((1, width), f32),
            pltpu.VMEM((2, row_count), jnp.int32),
            pltpu.VMEM((2, row_count), f32),
            pltpu.VMEM(out_weight.shape, bf),
            pltpu.VMEM(w_gate.shape[1:], bf),
            pltpu.VMEM(w_up.shape[1:], bf),
            pltpu.VMEM(w_down.shape[1:], bf),
            pltpu.VMEM((reach + SUBLANES, channels), f32),
            pltpu.VMEM((spn, SUBLANES, LANES), f32),
            pltpu.VMEM((spn * cap, row_count), bf),
            pltpu.VMEM((row_count, spn * cap), bf),
            pltpu.VMEM((reach + tok_rows, channels), f32),
            pltpu.VMEM((reach, channels), bf),
            pltpu.VMEM((reach, channels), bf),
            pltpu.VMEM((tpn, row_count, channels), bf),
            pltpu.VMEM((row_count, channels * tpn), bf),
            pltpu.VMEM((4, channels * tpn), f32),
            pltpu.VMEM((row_count, channels * tpn), bf),
            pltpu.VMEM((row_count, width), bf),
            pltpu.VMEM((pieces, height, width), bf),
            pltpu.VMEM((pieces, height, width), bf),
            pltpu.VMEM((pieces, tpn, height, width), bf),
            pltpu.VMEM((tpn * height, width), bf),
            pltpu.VMEM((spn, tpn, SUBLANES, LANES), f32),
            pltpu.VMEM((pieces, 2, height, width), f32),
            pltpu.VMEM((pieces, 2, height, width), bf),
            pltpu.VMEM((pieces, 2, height, width), bf),
            pltpu.VMEM((pieces, height, width), bf),
            pltpu.VMEM((pieces, height, width), bf),
            pltpu.VMEM((pieces, height, width), bf),
            pltpu.VMEM((tpn * height, hidden), bf),
            pltpu.VMEM((row_count, width), f32),
            pltpu.SemaphoreType.REGULAR((spn + 1,)),
            pltpu.SemaphoreType.REGULAR((spn + 1,)),
            dma((4,)),
            dma((11,)),
            dma((spn, tpn)),
            dma((spn, tpn)),
            dma((1,)),
            dma((1,)),
        ]
        + [dma((tpn,))] * 4
        + [dma((pieces,))] * 14,
        compiler_params=pltpu.CompilerParams(collective_id=0, has_side_effects=True),
    )(
        conv_value, conv_gate, kernel, conv_bias[None, :], ln_gain[None, :], ln_bias[None, :],
        out_gain[None, :], residual, moe_gain[None, :], expert_ids.T, expert_weights.T,
        out_weight, w_gate[0], w_up[0], w_down[0],
    )


def passed_along(block, axis, distance):
    devices = range(lax.axis_size(axis))
    route = [(i - distance, i) for i in devices if i - distance in devices]
    return lax.ppermute(block, axis, route)


def per_device(
    conv_value,
    conv_gate,
    kernel,
    conv_bias,
    ln_gain,
    ln_bias,
    out_gain,
    out_weight,
    residual,
    moe_gain,
    expert_ids,
    expert_weights,
    w_gate,
    w_up,
    w_down,
):
    tpn = lax.axis_size("tp")
    if lax.axis_size("sp") == GROUPS and tpn == 4:
        return fused_layer(
            conv_value, conv_gate, kernel, conv_bias, ln_gain, ln_bias, out_gain, out_weight, residual,
            moe_gain, expert_ids, expert_weights, w_gate, w_up, w_down,
        )
    tok_rows, channels = conv_value.shape
    reach_rows = kernel.shape[0] - 1
    full_channels = channels * lax.axis_size("tp")
    gated = (conv_value.astype(jnp.float32) * jax.nn.sigmoid(conv_gate.astype(jnp.float32))).astype(
        jnp.bfloat16
    )
    before = passed_along(gated[tok_rows - reach_rows :], "sp", 1)
    padded = jnp.concatenate([before, gated], axis=0)
    convolved = jnp.zeros((tok_rows, channels), jnp.float32) + conv_bias
    for offset in range(reach_rows + 1):
        convolved = convolved + padded[offset : offset + tok_rows].astype(jnp.float32) * kernel[
            offset
        ].astype(jnp.float32)
    totals = lax.psum((jnp.sum(convolved, axis=1), jnp.sum(convolved * convolved, axis=1)), "tp")
    average = (totals[0] / full_channels)[:, None]
    spread = (totals[1] / full_channels)[:, None] - average * average
    swished = jax.nn.silu((convolved - average) * lax.rsqrt(spread + EPSILON) * ln_gain + ln_bias)
    energy = lax.psum(jnp.sum(swished * swished, axis=1), "tp")
    branch = (swished * lax.rsqrt(energy / full_channels + EPSILON)[:, None] * out_gain).astype(
        jnp.bfloat16
    )
    row_count = tok_rows // lax.axis_size("tp")
    regrouped = lax.all_to_all(branch, "tp", split_axis=0, concat_axis=1, tiled=True)
    projected = jnp.dot(regrouped, out_weight, preferred_element_type=jnp.float32)
    hidden = (residual.astype(jnp.float32) + projected).astype(jnp.bfloat16)
    widened = hidden.astype(jnp.float32)
    normed = (
        widened * lax.rsqrt(jnp.mean(widened * widened, axis=1, keepdims=True) + EPSILON) * moe_gain
    ).astype(jnp.bfloat16)
    width = normed.shape[1]
    experts = lax.axis_size("sp") * lax.axis_size("tp")
    capacity = 2 * row_count // min(row_count, experts // 2)
    flat_ids = expert_ids.reshape(-1)
    onehot = (flat_ids[:, None] == jnp.arange(experts, dtype=jnp.int32)[None, :]).astype(jnp.int32)
    slot_rank = jnp.sum((jnp.cumsum(onehot, axis=0) - 1) * onehot, axis=1)
    position = flat_ids * capacity + slot_rank
    outgoing = (
        jnp.zeros((experts * capacity, width), jnp.bfloat16)
        .at[position]
        .set(jnp.repeat(normed, 2, axis=0))
    )
    outgoing = outgoing.reshape(experts, capacity, width)
    arriving = lax.all_to_all(outgoing, ("sp", "tp"), split_axis=0, concat_axis=0, tiled=True)
    flattened = arriving.reshape(-1, width)
    gate_part = jnp.dot(flattened, w_gate[0], preferred_element_type=jnp.float32)
    up_part = jnp.dot(flattened, w_up[0], preferred_element_type=jnp.float32)
    active = (jax.nn.silu(gate_part) * up_part).astype(jnp.bfloat16)
    result = jnp.dot(active, w_down[0], preferred_element_type=jnp.float32).astype(jnp.bfloat16)
    produced = result.reshape(arriving.shape)
    returned = lax.all_to_all(produced, ("sp", "tp"), split_axis=0, concat_axis=0, tiled=True)
    returned = returned.reshape(experts * capacity, width)
    picked = returned[position].reshape(row_count, 2, width)
    combined = jnp.sum(picked.astype(jnp.float32) * expert_weights[:, :, None], axis=1)
    return (widened + combined).astype(jnp.bfloat16)


def solution(mesh):
    in_specs = (
        P(("grp", "sp"), "tp"),
        P(("grp", "sp"), "tp"),
        P(None, "tp"),
        P("tp"),
        P("tp"),
        P("tp"),
        P("tp"),
        P(),
        P(("grp", "sp", "tp"), None),
        P(),
        P(("grp", "sp", "tp"), None),
        P(("grp", "sp", "tp"), None),
        P(("sp", "tp"), None, None),
        P(("sp", "tp"), None, None),
        P(("sp", "tp"), None, None),
    )
    out_specs = P(("grp", "sp", "tp"), None)
    return jax.shard_map(
        per_device, mesh=mesh, in_specs=in_specs, out_specs=out_specs, check_vma=False
    )
```

```python
import jax
import jax.numpy as jnp
from jax import lax
from jax.experimental import pallas as pl
from jax.experimental.pallas import tpu as pltpu
from jax.sharding import PartitionSpec as P

EPSILON = 1e-06
GROUPS = 4
SPLIT = 2
LANES = 128
SUBLANES = 8
MESH = pl.DeviceIdType.MESH
COLUMNS, LATE = (2, 7, 1, 0, 3, 4, 5, 6), 4
OUTER, OUTER_PARTS = (4, 3, 2, 5, 7, 6), 1
INNER, INNER_PARTS = (4, 5, 3, 6, 7, 2), 1
PLAN = (
    "f1 x0 z4 z3",
    "m0 c0 x1 x4",
    "z2 c4 z5 c1",
    "x3 h4 x2 h1",
    "b4 c3 z6 x5",
    "c5 z7 h3 h5",
    "b5 x6 b3 h0",
    "e4 c2 c6 x7",
    "h2 h6 b6 e5",
    "c7 e3 b2 h7",
    "b7 e6 b1 b0",
    "e2 e7 e1 e0",
)


def flipped(index, mask, size):
    total, bit = 0, 1
    while bit < size:
        total = total + ((index // bit + mask // bit) % 2) * bit
        bit *= 2
    return total


def gray(index):
    return flipped(index, index // 2, 4)


def layer_kernel(
    value_hbm, gate_hbm_in, kernel_hbm, bias_hbm, lgain_hbm, lbias_hbm, ogain_hbm, res_hbm, mgain_hbm, ids_hbm, shares_hbm,
    out_hbm, gate_hbm, up_hbm, down_hbm, result,
    value, gate, kernel, params, residual, moe_gain, ids, shares,
    w_out, w_gate, w_up, w_down, taps, meta, pick, unpick, padded, halo_out, halo_in, conv, wide, gains, branch, hid,
    send, back, rows, normed, weights, own, half_out, half_in, cross_out, cross_in, final, act, total,
    low, high, load_sem, in_sem, meta_s, meta_r, halo_s, halo_r, gain_s, gain_r, group_s, group_r,
    z_s, z_r, pair_s, pair_r, x_s, x_r, via_s, via_r,
    half_s, half_r, cross_s, cross_r, back_s, back_r,
):
    spn, tpn = weights.shape[:2]
    pieces, _, height, width = rows.shape
    cap = height * SPLIT
    last = pieces - 1
    me_z, me_t = lax.axis_index("sp"), lax.axis_index("tp")
    pair, across = flipped(me_t, 1, tpn), flipped(me_t, 2, tpn)
    hidden = w_gate.shape[1]
    tok_rows, channels = value.shape
    row_count = tok_rows // tpn
    full = channels * tpn
    reach = padded.shape[0] - tok_rows
    tap_count = kernel.shape[0]
    f32, bf = jnp.float32, jnp.bfloat16

    def to(z, t):
        return {"sp": z, "tp": t}

    def copy(src, dst, s, r, z, t):
        return pltpu.make_async_remote_copy(
            src_ref=src, dst_ref=dst, send_sem=s, recv_sem=r, device_id=to(z, t), device_id_type=MESH
        )

    peers = [(q, r) for q in range(spn) for r in range(tpn) if q or r]
    below, above = me_z > 0, me_z < spn - 1
    barrier = pltpu.get_barrier_semaphore()

    def tell(semaphore, z, t):
        pl.semaphore_signal(semaphore, inc=1, device_id=to(z, t), device_id_type=MESH)

    for r in range(1, tpn):
        tell(barrier, me_z, flipped(me_t, r, tpn))

    @pl.when(below)
    def _():
        tell(barrier, me_z - 1, me_t)

    @pl.when(above)
    def _():
        tell(barrier, me_z + 1, me_t)

    def pass_on(d):
        @pl.when(me_z >= d)
        def _():
            pl.semaphore_wait(low.at[d], 1)

            @pl.when(above)
            def _():
                tell(low.at[d + 1], me_z + 1, me_t)

        @pl.when(me_z + d < spn)
        def _():
            pl.semaphore_wait(high.at[d], 1)

            @pl.when(below)
            def _():
                tell(high.at[d + 1], me_z - 1, me_t)

    inputs = [
        pltpu.make_async_copy(a, b, in_sem.at[i])
        for i, (a, b) in enumerate((
            (value_hbm, value), (gate_hbm_in, gate), (kernel_hbm, kernel), (bias_hbm, params.at[pl.ds(3, 1)]),
            (lgain_hbm, params.at[pl.ds(0, 1)]), (lbias_hbm, params.at[pl.ds(1, 1)]),
            (ogain_hbm, params.at[pl.ds(2, 1)]), (ids_hbm, ids), (shares_hbm, shares),
            (res_hbm, residual), (mgain_hbm, moe_gain),
        ))
    ]
    loads = [
        pltpu.make_async_copy(a, b, load_sem.at[i])
        for i, (a, b) in enumerate(((out_hbm, w_out), (gate_hbm, w_gate), (up_hbm, w_up), (down_hbm, w_down)))
    ]
    for load in inputs:
        load.start()

    for load in inputs[:7]:
        load.wait()
    for load in loads:
        load.start()
    taps[:tap_count, :] = kernel[...].astype(f32)
    gated = (value[...].astype(f32) / (1.0 + jnp.exp(-gate[...].astype(f32)))).astype(bf)
    padded[reach:, :] = gated.astype(f32)
    halo_out[...] = gated[tok_rows - reach :]

    mine = pl.ds(pl.multiple_of(me_t * channels, channels), channels)

    def halo_copy(z):
        return copy(halo_out, halo_in, halo_s.at[0], halo_r.at[0], z, me_t)

    def gain_copy(r):
        return copy(params, gains.at[:, mine], gain_s.at[r], gain_r.at[r], me_z, flipped(me_t, r, tpn))

    def group_copy(t, low, high):
        span = pl.ds(low, high - low)
        r = flipped(me_t, t, tpn)
        return copy(conv.at[t, span], wide.at[span, mine], group_s.at[r], group_r.at[r], me_z, t)

    def z_copy(k, cols=pl.ds(0, width)):
        return copy(
            send.at[k, :, cols], rows.at[k, 0, :, cols], z_s.at[k], z_r.at[k],
            flipped(me_z, gray(k // SPLIT), spn), me_t,
        )

    def meta_copy(q, r):
        return copy(
            meta.at[q], weights.at[q, r], meta_s.at[q, r], meta_r.at[q, r],
            flipped(me_z, gray(q), spn), flipped(me_t, r, tpn),
        )

    def pair_copy(k):
        return copy(rows.at[k, 0], rows.at[k, 1], pair_s.at[k], pair_r.at[k], me_z, pair)

    def x_copy(k, cols=pl.ds(0, width)):
        return copy(
            rows.at[k, 0, :, cols], rows.at[k, 2, :, cols], x_s.at[k], x_r.at[k], me_z, across
        )

    def via_copy(k):
        return copy(rows.at[k, 2], rows.at[k, 3], via_s.at[k], via_r.at[k], me_z, pair)

    def half_copy(k):
        return copy(half_out.at[k], half_in.at[k], half_s.at[k], half_r.at[k], me_z, pair)

    def cross_copy(k):
        return copy(cross_out.at[k], cross_in.at[k], cross_s.at[k], cross_r.at[k], me_z, across)

    def back_copy(k):
        return copy(
            final.at[k], back.at[COLUMNS.index(k)], back_s.at[k], back_r.at[k], flipped(me_z, gray(k // SPLIT), spn), me_t
        )

    def convolve(block, first, count):
        start = pl.multiple_of(block * row_count + first, SUBLANES)
        for c in range(0, channels, LANES):
            window = padded[pl.ds(start, count + reach), c : c + LANES]
            sums = jnp.zeros((count, LANES), f32) + params[3:4, c : c + LANES]
            for b in range(SUBLANES):
                extent = count + (SUBLANES if b else 0)
                group = None
                for a in range(0, reach + 1, SUBLANES):
                    tap = a + b - (reach - tap_count + 1)
                    if 0 <= tap < tap_count:
                        term = window[a : a + extent] * taps[tap : tap + 1, c : c + LANES]
                        group = term if group is None else group + term
                sums = sums + group[b : b + count]
            conv[block, first : first + count, c : c + LANES] = sums.astype(bf)

    side = me_t // 2
    for j, b in enumerate((2, 3, 1, 0)):
        block = b + side * (3 - 2 * b)
        edge = b in (0, 3)
        convolve(block, reach, row_count - reach)
        if edge:
            @pl.when(block != 0)
            def _():
                convolve(block, 0, reach)
        else:
            convolve(block, 0, reach)
        if j == 0:
            pl.semaphore_wait(barrier, tpn - 1 + jnp.where(below & above, 2, 1))

            @pl.when(above)
            def _():
                halo_copy(me_z + 1).start()
                tell(low.at[1], me_z + 1, me_t)

            @pl.when(below)
            def _():
                tell(high.at[1], me_z - 1, me_t)

            for r in range(1, tpn):
                gain_copy(r).start()

        if edge:
            @pl.when((block != me_t) & (block != 0))
            def _():
                group_copy(block, 0, row_count).start()

            @pl.when((block != me_t) & (block == 0))
            def _():
                group_copy(block, reach, row_count).start()
        else:
            @pl.when(block != me_t)
            def _():
                group_copy(block, 0, row_count).start()

    @pl.when(me_z == 0)
    def _():
        padded[:reach, :] = jnp.zeros((reach, channels), f32)

    @pl.when(me_z > 0)
    def _():
        halo_copy(me_z - 1).wait_recv()
        padded[:reach, :] = halo_in[...].astype(f32)

    convolve(0, 0, reach)

    @pl.when(me_t != 0)
    def _():
        group_copy(0, 0, reach).start()

    wide[:, mine] = conv[me_t]
    gains[:, mine] = params[...]

    pass_on(1)
    for load in inputs[7:9]:
        load.wait()
    square = (row_count, row_count)
    down, along = (lax.broadcasted_iota(jnp.int32, square, d) for d in (0, 1))

    def upright(line):
        return jnp.sum(
            jnp.where(down == along, jnp.broadcast_to(line, square), jnp.zeros((), line.dtype)),
            axis=1, keepdims=True,
        )

    def distance(number):
        mask = jnp.bitwise_xor(number, me_z)
        return jnp.bitwise_xor(mask, lax.div(mask, 2))

    def place(number, order):
        found = distance(number) * SPLIT + lax.div(order, height)
        column = sum(jnp.where(found == k, c, 0) for c, k in enumerate(COLUMNS))
        return column * height + lax.rem(order, height)

    group_row = jnp.broadcast_to(lax.div(ids[0:1, :], tpn), square)
    group = jnp.broadcast_to(upright(group_row[0:1, :]), square)
    same = group == group_row
    rank = jnp.sum(jnp.where(same & (along < down), 1, 0), axis=1, keepdims=True)
    rank_row = jnp.sum(jnp.where(same & (down < along), 1, 0), axis=0, keepdims=True)
    slot = place(group[:, 0:1], rank)
    slot_row = place(group_row[0:1, :], rank_row)
    slots = spn * cap
    pick[...] = jnp.where(
        lax.broadcasted_iota(jnp.int32, (slots, row_count), 0) == slot_row, 1.0, 0.0
    ).astype(bf)
    unpick[...] = jnp.where(
        lax.broadcasted_iota(jnp.int32, (row_count, slots), 1) == slot, 1.0, 0.0
    ).astype(bf)
    lane = lax.broadcasted_iota(jnp.int32, (row_count, LANES), 1)
    experts = lax.rem(ids[...], tpn)
    meta[...] = jnp.zeros_like(meta)
    by_expert = [
        upright(jnp.sum(jnp.where(experts == e, shares[...], 0.0), axis=0, keepdims=True))
        for e in range(tpn)
    ]
    for q in range(spn):
        here = (distance(group[:, 0:1]) == q) & (lane == rank)
        for e in range(tpn):
            share = by_expert[e]
            meta[q, e : e + 1, :] = jnp.sum(jnp.where(here, share, 0.0), axis=0, keepdims=True)
    weights[0, 0] = meta[0]
    for d in range(2, spn):
        pass_on(d)
    for q, r in peers:
        meta_copy(q, r).start()

    for load in inputs[9:]:
        load.wait()
    loads[0].wait()
    for r in range(1, tpn):
        gain_copy(r).wait_recv()
    for r in range(1, tpn):
        t = flipped(me_t, r, tpn)
        group_copy(t, 0, row_count).wait_recv()

    part = min(row_count, 32)
    for first in range(0, row_count, part):
        v = wide[first : first + part, :].astype(f32)
        average = jnp.sum(v, axis=1, keepdims=True) / full
        spread = jnp.sum(v * v, axis=1, keepdims=True) / full - average * average
        v = (v - average) * lax.rsqrt(spread + EPSILON) * gains[0:1, :] + gains[1:2, :]
        v = v / (1.0 + jnp.exp(-v))
        energy = jnp.sum(v * v, axis=1, keepdims=True) / full
        branch[first : first + part, :] = (v * lax.rsqrt(energy + EPSILON) * gains[2:3, :]).astype(bf)

    tile = min(hidden, 512)
    inner = (me_z > 0) & (me_z < spn - 1)

    def project(c, carry):
        cols = pl.ds(pl.multiple_of(c * tile, tile), tile)
        h = residual[:, cols].astype(f32) + jnp.dot(
            branch[...], w_out[:, cols], preferred_element_type=f32
        )
        h = h.astype(bf)
        hid[:, cols] = h
        picked = jnp.dot(pick[...], h, preferred_element_type=f32).astype(bf)
        for k in range(pieces):
            at = COLUMNS.index(k) * height
            taken = picked[at : at + height]
            if k < SPLIT:
                rows[k, 0, :, cols] = taken
            else:
                send[k, :, cols] = taken
        x_copy(0, cols).start()

        @pl.when(inner)
        def _():
            for k in INNER[:INNER_PARTS]:
                z_copy(k, cols).start()

        @pl.when(jnp.logical_not(inner))
        def _():
            for k in OUTER[:OUTER_PARTS]:
                z_copy(k, cols).start()

        return carry

    for c in range(width // tile):
        project(c, 0)
    pair_copy(0).start()

    @pl.when(inner)
    def _():
        for k in INNER[INNER_PARTS:]:
            z_copy(k).start()

    @pl.when(jnp.logical_not(inner))
    def _():
        for k in OUTER[OUTER_PARTS:]:
            z_copy(k).start()


    row_of, lane_of = (lax.broadcasted_iota(jnp.int32, (height, LANES), d) for d in (0, 1))

    def compute(k):
        strip = height // 2
        for r in range(tpn):
            for first in range(0, height, strip):
                h = rows[k, r, first : first + strip].astype(f32)
                level = lax.rsqrt(jnp.sum(h * h, axis=1, keepdims=True) / width + EPSILON)
                low = r * height + first
                normed[low : low + strip] = (h * level * moe_gain[...]).astype(bf)
        x = normed[...]
        diagonal = lane_of == row_of + (k % SPLIT) * height
        for c in range(0, hidden, 256):
            g = jnp.dot(x, w_gate[:, c : c + 256], preferred_element_type=jnp.float32)
            u = jnp.dot(x, w_up[:, c : c + 256], preferred_element_type=jnp.float32)
            act[:, c : c + 256] = (g / (1.0 + jnp.exp(-g)) * u).astype(jnp.bfloat16)
        a = act[...]
        scales = [
            jnp.sum(jnp.where(diagonal, weights[k // SPLIT, r, pl.ds(me_t, 1), :], 0.0), axis=1, keepdims=True)
            for r in range(tpn)
        ]

        def column(c, carry):
            cols = pl.ds(pl.multiple_of(c * tile, tile), tile)
            res = jnp.dot(a, w_down[:, cols], preferred_element_type=jnp.float32).astype(jnp.bfloat16)
            res = res.astype(jnp.float32)
            parts = [res[r * height : (r + 1) * height] * scales[r] for r in range(tpn)]
            half_out[k, 0, :, cols] = parts[1].astype(jnp.bfloat16)
            half_out[k, 1, :, cols] = parts[3].astype(jnp.bfloat16)
            own[k, 0, :, cols] = parts[0]
            own[k, 1, :, cols] = parts[2]
            return carry

        lax.fori_loop(0, width // tile, column, 0)

    def first(k):
        x_copy(k).start()
        pair_copy(k).start()

    def forward(k):
        z_copy(k).wait_recv()
        first(k)

    def relay(k):
        x_copy(k).wait_recv()
        via_copy(k).start()

    def run(k):
        pair_copy(k).wait_recv()
        via_copy(k).wait_recv()
        compute(k)
        half_copy(k).start()

    def halve(k):
        half_copy(k).wait_recv()
        cross_out[k] = (own[k, 1] + half_in[k, 1].astype(jnp.float32)).astype(jnp.bfloat16)

    def cross(k):
        cross_copy(k).start()

    def finish(k):
        cross_copy(k).wait_recv()
        ready = (
            own[k, 0] + half_in[k, 0].astype(jnp.float32) + cross_in[k].astype(jnp.float32)
        ).astype(jnp.bfloat16)
        if k < SPLIT:
            back[COLUMNS.index(k)] = ready
        else:
            final[k] = ready
            back_copy(k).start()

    def arrive(k):
        for q, r in peers:
            meta_copy(q, r).wait_recv()
        for load in loads[1:]:
            load.wait()

    acts = {"m": arrive, "f": first, "z": forward, "x": relay, "c": run, "h": halve, "b": cross, "e": finish}
    for line in PLAN:
        for word in line.split():
            acts[word[0]](int(word[1:]))

    edge = LATE * height
    for k in COLUMNS[LATE:]:
        if k >= SPLIT:
            back_copy(k).wait_recv()
    for c in range(0, width, tile):
        moved = back[LATE:, :, c : c + tile].reshape((pieces - LATE) * height, tile)
        total[:, c : c + tile] = hid[:, c : c + tile].astype(f32) + jnp.dot(
            unpick[:, edge:], moved, preferred_element_type=f32
        )
    for k in COLUMNS[:LATE]:
        if k >= SPLIT:
            back_copy(k).wait_recv()

    for c in range(0, width, tile):
        moved = back[:LATE, :, c : c + tile].reshape(edge, tile)
        result[:, c : c + tile] = (
            total[:, c : c + tile] + jnp.dot(unpick[:, :edge], moved, preferred_element_type=f32)
        ).astype(bf)

    @pl.when(me_z < spn - 1)
    def _():
        halo_copy(me_z + 1).wait_send()

    for r in range(1, tpn):
        gain_copy(r).wait_send()
        group_copy(flipped(me_t, r, tpn), 0, row_count).wait_send()
    for q, r in peers:
        meta_copy(q, r).wait_send()
    for k in range(pieces):
        for make in (x_copy, pair_copy, via_copy, half_copy, cross_copy):
            make(k).wait_send()
    for k in range(SPLIT, pieces):
        z_copy(k).wait_send()
        back_copy(k).wait_send()


def fused_layer(
    conv_value,
    conv_gate,
    kernel,
    conv_bias,
    ln_gain,
    ln_bias,
    out_gain,
    out_weight,
    residual,
    moe_gain,
    expert_ids,
    expert_weights,
    w_gate,
    w_up,
    w_down,
):
    spn, tpn = lax.axis_size("sp"), lax.axis_size("tp")
    tok_rows, channels = conv_value.shape
    row_count, width = residual.shape
    hidden = w_gate.shape[2]
    capacity = 2 * row_count // min(row_count, spn * tpn // 2)
    cap = tpn * capacity // 2
    pieces, height = spn * SPLIT, cap // SPLIT
    reach = -(-(kernel.shape[0] - 1) // SUBLANES) * SUBLANES
    bf, f32, dma = jnp.bfloat16, jnp.float32, pltpu.SemaphoreType.DMA
    hbm = pl.BlockSpec(memory_space=pl.ANY)
    return pl.pallas_call(
        layer_kernel,
        out_shape=pltpu.VMEM((row_count, width), bf),
        in_specs=[hbm] * 15,
        out_specs=pl.BlockSpec(memory_space=pltpu.VMEM),
        scratch_shapes=[
            pltpu.VMEM(conv_value.shape, bf),
            pltpu.VMEM(conv_gate.shape, bf),
            pltpu.VMEM(kernel.shape, bf),
            pltpu.VMEM((4, channels), f32),
            pltpu.VMEM(residual.shape, bf),
            pltpu.VMEM((1, width), f32),
            pltpu.VMEM((2, row_count), jnp.int32),
            pltpu.VMEM((2, row_count), f32),
            pltpu.VMEM(out_weight.shape, bf),
            pltpu.VMEM(w_gate.shape[1:], bf),
            pltpu.VMEM(w_up.shape[1:], bf),
            pltpu.VMEM(w_down.shape[1:], bf),
            pltpu.VMEM((reach + SUBLANES, channels), f32),
            pltpu.VMEM((spn, SUBLANES, LANES), f32),
            pltpu.VMEM((spn * cap, row_count), bf),
            pltpu.VMEM((row_count, spn * cap), bf),
            pltpu.VMEM((reach + tok_rows, channels), f32),
            pltpu.VMEM((reach, channels), bf),
            pltpu.VMEM((reach, channels), bf),
            pltpu.VMEM((tpn, row_count, channels), bf),
            pltpu.VMEM((row_count, channels * tpn), bf),
            pltpu.VMEM((4, channels * tpn), f32),
            pltpu.VMEM((row_count, channels * tpn), bf),
            pltpu.VMEM((row_count, width), bf),
            pltpu.VMEM((pieces, height, width), bf),
            pltpu.VMEM((pieces, height, width), bf),
            pltpu.VMEM((pieces, tpn, height, width), bf),
            pltpu.VMEM((tpn * height, width), bf),
            pltpu.VMEM((spn, tpn, SUBLANES, LANES), f32),
            pltpu.VMEM((pieces, 2, height, width), f32),
            pltpu.VMEM((pieces, 2, height, width), bf),
            pltpu.VMEM((pieces, 2, height, width), bf),
            pltpu.VMEM((pieces, height, width), bf),
            pltpu.VMEM((pieces, height, width), bf),
            pltpu.VMEM((pieces, height, width), bf),
            pltpu.VMEM((tpn * height, hidden), bf),
            pltpu.VMEM((row_count, width), f32),
            pltpu.SemaphoreType.REGULAR((spn + 1,)),
            pltpu.SemaphoreType.REGULAR((spn + 1,)),
            dma((4,)),
            dma((11,)),
            dma((spn, tpn)),
            dma((spn, tpn)),
            dma((1,)),
            dma((1,)),
        ]
        + [dma((tpn,))] * 4
        + [dma((pieces,))] * 14,
        compiler_params=pltpu.CompilerParams(collective_id=0, has_side_effects=True),
    )(
        conv_value, conv_gate, kernel, conv_bias[None, :], ln_gain[None, :], ln_bias[None, :],
        out_gain[None, :], residual, moe_gain[None, :], expert_ids.T, expert_weights.T,
        out_weight, w_gate[0], w_up[0], w_down[0],
    )


def passed_along(block, axis, distance):
    devices = range(lax.axis_size(axis))
    route = [(i - distance, i) for i in devices if i - distance in devices]
    return lax.ppermute(block, axis, route)


def per_device(
    conv_value,
    conv_gate,
    kernel,
    conv_bias,
    ln_gain,
    ln_bias,
    out_gain,
    out_weight,
    residual,
    moe_gain,
    expert_ids,
    expert_weights,
    w_gate,
    w_up,
    w_down,
):
    tpn = lax.axis_size("tp")
    if lax.axis_size("sp") == GROUPS and tpn == 4:
        return fused_layer(
            conv_value, conv_gate, kernel, conv_bias, ln_gain, ln_bias, out_gain, out_weight, residual,
            moe_gain, expert_ids, expert_weights, w_gate, w_up, w_down,
        )
    tok_rows, channels = conv_value.shape
    reach_rows = kernel.shape[0] - 1
    full_channels = channels * lax.axis_size("tp")
    gated = (conv_value.astype(jnp.float32) * jax.nn.sigmoid(conv_gate.astype(jnp.float32))).astype(
        jnp.bfloat16
    )
    before = passed_along(gated[tok_rows - reach_rows :], "sp", 1)
    padded = jnp.concatenate([before, gated], axis=0)
    convolved = jnp.zeros((tok_rows, channels), jnp.float32) + conv_bias
    for offset in range(reach_rows + 1):
        convolved = convolved + padded[offset : offset + tok_rows].astype(jnp.float32) * kernel[
            offset
        ].astype(jnp.float32)
    totals = lax.psum((jnp.sum(convolved, axis=1), jnp.sum(convolved * convolved, axis=1)), "tp")
    average = (totals[0] / full_channels)[:, None]
    spread = (totals[1] / full_channels)[:, None] - average * average
    swished = jax.nn.silu((convolved - average) * lax.rsqrt(spread + EPSILON) * ln_gain + ln_bias)
    energy = lax.psum(jnp.sum(swished * swished, axis=1), "tp")
    branch = (swished * lax.rsqrt(energy / full_channels + EPSILON)[:, None] * out_gain).astype(
        jnp.bfloat16
    )
    row_count = tok_rows // lax.axis_size("tp")
    regrouped = lax.all_to_all(branch, "tp", split_axis=0, concat_axis=1, tiled=True)
    projected = jnp.dot(regrouped, out_weight, preferred_element_type=jnp.float32)
    hidden = (residual.astype(jnp.float32) + projected).astype(jnp.bfloat16)
    widened = hidden.astype(jnp.float32)
    normed = (
        widened * lax.rsqrt(jnp.mean(widened * widened, axis=1, keepdims=True) + EPSILON) * moe_gain
    ).astype(jnp.bfloat16)
    width = normed.shape[1]
    experts = lax.axis_size("sp") * lax.axis_size("tp")
    capacity = 2 * row_count // min(row_count, experts // 2)
    flat_ids = expert_ids.reshape(-1)
    onehot = (flat_ids[:, None] == jnp.arange(experts, dtype=jnp.int32)[None, :]).astype(jnp.int32)
    slot_rank = jnp.sum((jnp.cumsum(onehot, axis=0) - 1) * onehot, axis=1)
    position = flat_ids * capacity + slot_rank
    outgoing = (
        jnp.zeros((experts * capacity, width), jnp.bfloat16)
        .at[position]
        .set(jnp.repeat(normed, 2, axis=0))
    )
    outgoing = outgoing.reshape(experts, capacity, width)
    arriving = lax.all_to_all(outgoing, ("sp", "tp"), split_axis=0, concat_axis=0, tiled=True)
    flattened = arriving.reshape(-1, width)
    gate_part = jnp.dot(flattened, w_gate[0], preferred_element_type=jnp.float32)
    up_part = jnp.dot(flattened, w_up[0], preferred_element_type=jnp.float32)
    active = (jax.nn.silu(gate_part) * up_part).astype(jnp.bfloat16)
    result = jnp.dot(active, w_down[0], preferred_element_type=jnp.float32).astype(jnp.bfloat16)
    produced = result.reshape(arriving.shape)
    returned = lax.all_to_all(produced, ("sp", "tp"), split_axis=0, concat_axis=0, tiled=True)
    returned = returned.reshape(experts * capacity, width)
    picked = returned[position].reshape(row_count, 2, width)
    combined = jnp.sum(picked.astype(jnp.float32) * expert_weights[:, :, None], axis=1)
    return (widened + combined).astype(jnp.bfloat16)


def solution(mesh):
    in_specs = (
        P(("grp", "sp"), "tp"),
        P(("grp", "sp"), "tp"),
        P(None, "tp"),
        P("tp"),
        P("tp"),
        P("tp"),
        P("tp"),
        P(),
        P(("grp", "sp", "tp"), None),
        P(),
        P(("grp", "sp", "tp"), None),
        P(("grp", "sp", "tp"), None),
        P(("sp", "tp"), None, None),
        P(("sp", "tp"), None, None),
        P(("sp", "tp"), None, None),
    )
    out_specs = P(("grp", "sp", "tp"), None)
    return jax.shard_map(
        per_device, mesh=mesh, in_specs=in_specs, out_specs=out_specs, check_vma=False
    )
```
